128 devices in a mesh: sp: 16 (over z, y), tp: 8 (over x, core).
Axes of the slice: x: 4, y: 4, z: 4, core: 2. Of those that a mesh axis runs over, the one named last changes fastest.
Arguments:
- inputs: bfloat16 [16384, 2048], P('sp'), may hold values from -6 to 6
- norm_gain: float32 [3, 2048], replicated, may hold values from 0.1 to 1.9
- query_weight: bfloat16 [3, 2048, 1024], P(None, 'sp', 'tp'), may hold values from -64 to 64
- key_weight: bfloat16 [3, 2048, 512], P(None, 'sp', 'tp'), may hold values from -4 to 4
- value_weight: bfloat16 [3, 2048, 512], P(None, 'sp', 'tp'), may hold values from -0.125 to 0.125
- output_weight: bfloat16 [3, 2048, 1024], P(None, 'sp', 'tp'), may hold values from -0.1875 to 0.1875
- sink_logit: float32 [3, 16], P(None, 'tp'), may hold values from 2 to 7
- final_gain: float32 [2048], replicated, may hold values from 0.1 to 1.9
Outputs:
- result: float32 [16384, 2048], P(('sp', 'tp'))
The draws below stay inside these ranges and needn't reach their ends.
All inputs are finite; a program needn't handle non-finite values.
Results may differ from the reference program's by a relative error of at most 0.015.
Values may be sent and summed in bfloat16 or wider, within the bound.
A program may use at most 64 MiB of HBM per device.

```python
import jax
import jax.numpy as jnp
from jax import lax

D = 2048
HEADS = 16
KV_HEADS = 8
HEAD_DIM = 64
WINDOW = 128
LAYERS = 3
TOK_DEV = 1024
SEQ = 16384


def shared_keys(key):
    base_key = jax.random.fold_in(key, 7)
    shape = (LAYERS, D, KV_HEADS * HEAD_DIM)
    return jnp.clip(jax.random.normal(base_key, shape, jnp.float32), -4.0, 4.0)


def draw_key_weight(key, part):
    return shared_keys(key).astype(jnp.bfloat16)


def draw_query_weight(key, part):
    base_key = jax.random.fold_in(key, 13)
    drawn = jax.random.normal(base_key, (LAYERS, D, HEADS * HEAD_DIM), jnp.float32)
    return jnp.clip(drawn, -4.0, 4.0).astype(jnp.bfloat16)


def level_of(key, dims, shards, smallest, high):
    loudness = 1.0
    for position, parts in shards:
        draws = jax.random.uniform(jax.random.fold_in(jax.random.fold_in(key, 6), position), (parts,), jnp.float32, smallest / len(shards), high / len(shards))
        loudness = loudness * jnp.repeat(jnp.exp(draws), dims[position] // parts).reshape((-1,) + (1,) * (len(dims) - 1 - position))
    return loudness


def bell_draw(own_key, extent, deviation, bound, cuts=(), kind=jnp.bfloat16):
    values = jax.random.normal(own_key, extent, jnp.float32) * deviation
    if len(cuts) > 0:
        values = level_of(own_key, extent, cuts, -0.22, 0.18) * values
    return jnp.clip(values, min=-bound, max=bound).astype(kind)


def setup_inputs(seed: int = 0) -> dict:
    streams_of = jax.random.split(jax.random.key(seed), 9)
    inputs = bell_draw(streams_of[0], (SEQ, D), 1.0, 6.0, ((0, 16),))
    norm_gain = jnp.clip(1.0 + 0.18 * jax.random.normal(streams_of[1], (LAYERS, D), jnp.float32), 0.1, 1.9)
    query_weight = draw_query_weight(jax.random.fold_in(streams_of[8], 71), 0)
    key_weight = draw_key_weight(jax.random.fold_in(streams_of[8], 71), 0)
    value_weight = bell_draw(streams_of[4], (LAYERS, D, KV_HEADS * HEAD_DIM), D ** -0.5, 0.125, ((1, 16), (2, 8)))
    output_weight = bell_draw(streams_of[5], (LAYERS, D, HEADS * HEAD_DIM), (HEADS * HEAD_DIM) ** -0.5, 0.1875, ((1, 16), (2, 8)))
    sink_logit = jnp.clip(2.0 + 5.0 * jax.random.uniform(streams_of[6], (LAYERS, HEADS), jnp.float32) ** level_of(streams_of[6], (LAYERS, HEADS), ((1, 8),), -0.2, 0.2), 2.0, 7.0)
    final_gain = jnp.clip(1.0 + 0.18 * jax.random.normal(streams_of[7], (D,), jnp.float32), 0.1, 1.9)
    return {"inputs": inputs, "norm_gain": norm_gain, "query_weight": query_weight, "key_weight": key_weight, "value_weight": value_weight, "output_weight": output_weight, "sink_logit": sink_logit, "final_gain": final_gain}


EPS = 1e-06

def norm_rows(values, gain):
    wide_values = values.astype(jnp.float32)
    inv_root = lax.rsqrt(lax.optimization_barrier(jnp.mean(wide_values * wide_values, axis=-1, keepdims=True)) + EPS)
    return wide_values * inv_root * gain

def rotate(values, places):
    half_dim = values.shape[-1] // 2
    inverse = 10000.0 ** (-jnp.arange(half_dim).astype(jnp.float32) / half_dim)
    angles = places[:, None] * inverse[None, :]
    cosine_table = jnp.cos(angles)[:, None, :]
    sine_table = jnp.sin(angles)[:, None, :]
    front_half = values[..., :half_dim]
    back_half = values[..., half_dim:]
    return jnp.concatenate([front_half * cosine_table - back_half * sine_table, back_half * cosine_table + front_half * sine_table], axis=-1)

def attend(queries, key_rows, value_rows, sink_row, allowed):
    scores = jnp.einsum('qkgd,skd->kgqs', queries.astype(jnp.float32), key_rows.astype(jnp.float32)) * queries.shape[-1] ** (-0.5)
    scores = jnp.where(allowed[None, None], scores, -jnp.inf)
    sink_col = sink_row[:, :, None]
    largest = jnp.maximum(lax.optimization_barrier(jnp.max(scores, axis=-1)), sink_col)
    powers = jnp.exp(scores - largest[..., None])
    denominator = lax.optimization_barrier(jnp.sum(powers, axis=-1)) + jnp.exp(sink_col - largest)
    weights = (powers / denominator[..., None]).astype(jnp.bfloat16)
    blended = jnp.einsum('kgqs,skd->qkgd', weights.astype(jnp.float32), value_rows.astype(jnp.float32))
    return blended.astype(jnp.bfloat16)

def reference(inputs, norm_gain, query_weight, key_weight, value_weight, output_weight, sink_logit, final_gain):
    seq_total = inputs.shape[0]
    blocks = seq_total // TOK_DEV
    per_group = HEADS // KV_HEADS
    places = jnp.arange(seq_total).astype(jnp.float32)
    current = inputs
    for layer in range(LAYERS):
        normed = norm_rows(current, norm_gain[layer]).astype(jnp.bfloat16)
        query_raw = jnp.dot(normed, query_weight[layer], preferred_element_type=jnp.float32) * float(D) ** (-0.5)
        key_raw = jnp.dot(normed, key_weight[layer], preferred_element_type=jnp.float32) * float(D) ** (-0.5)
        value_raw = jnp.dot(normed, value_weight[layer], preferred_element_type=jnp.float32)
        queries = rotate(query_raw.reshape(seq_total, HEADS, HEAD_DIM), places).astype(jnp.bfloat16)
        queries = queries.reshape(seq_total, KV_HEADS, per_group, HEAD_DIM)
        key_rot = rotate(key_raw.reshape(seq_total, KV_HEADS, HEAD_DIM), places).astype(jnp.bfloat16)
        value_all = value_raw.astype(jnp.bfloat16).reshape(seq_total, KV_HEADS, HEAD_DIM)
        padding = ((WINDOW, WINDOW), (0, 0), (0, 0))
        pad_keys = jnp.pad(key_rot, padding)
        pad_values = jnp.pad(value_all, padding)
        sink_row = sink_logit[layer].reshape(KV_HEADS, per_group)

        def one_block(block_index):
            first_row = block_index * TOK_DEV
            block_queries = lax.dynamic_slice_in_dim(queries, first_row, TOK_DEV, 0)
            block_keys = lax.dynamic_slice_in_dim(pad_keys, first_row, TOK_DEV + 2 * WINDOW, 0)
            block_values = lax.dynamic_slice_in_dim(pad_values, first_row, TOK_DEV + 2 * WINDOW, 0)
            query_pos = first_row + jnp.arange(TOK_DEV, dtype=jnp.int32)
            key_pos = first_row - WINDOW + jnp.arange(TOK_DEV + 2 * WINDOW, dtype=jnp.int32)
            allowed = (jnp.abs(key_pos[None, :] - query_pos[:, None]) <= WINDOW) & (key_pos[None, :] >= 0) & (key_pos[None, :] < seq_total)
            return attend(block_queries, block_keys, block_values, sink_row, allowed)
        attended = lax.map(one_block, jnp.arange(blocks, dtype=jnp.int32)).reshape(seq_total, HEADS * HEAD_DIM)
        current = jnp.dot(attended, output_weight[layer].T, preferred_element_type=jnp.float32).astype(jnp.bfloat16)
    return norm_rows(current, final_gain)
```

```python
import functools

import jax
import jax.numpy as jnp
from jax import lax
from jax.experimental import pallas as pl
from jax.experimental.pallas import tpu as pltpu
from jax.sharding import PartitionSpec as P

D = 2048
HEAD_DIM = 64
WINDOW = 128
LAYERS = 3
EPS = 1e-06
BLK = 128
RING = 4
SEQ = 16384
MASKED = -1e30
MESH = pl.DeviceIdType.MESH
F32 = jnp.float32
BF16 = jnp.bfloat16

ROTATIONS = (("x", "y", "z"), ("y", "z", "x"), ("z", "x", "y"))
DIMS = ("x", "z", "y")
STAGES = ((0, 0, 3), (1, 0, 1), (1, 1, 3), (2, 0, 1), (2, 1, 2), (2, 2, 3))
N_IDS = len(STAGES) * 3 * 6


def mod4(v):
    return lax.rem(v + 2 * RING, RING)


def kernel(
    inputs, q_w, k_w, v_w, o_w, norm_gain, final_gain, sink_tile, q_cos, q_sin, kv_cos, kv_sin,
    out,
    g_q, g_kv, g_o, staged, normed, kv_rows, q_rows, att, part_own, part_send, part_recv, bias, sinks,
    send_sem, recv_sem, local_sem, halo_send, halo_recv, part_ssem, part_rsem, norm_ssem, norm_rsem,
    sink_ssem, sink_rsem,
):
    sp, tp = lax.axis_index("sp"), lax.axis_index("tp")
    z, y = sp // RING, lax.rem(sp, RING)
    x, c = tp // 2, lax.rem(tp, 2)
    at = {"x": x, "y": y, "z": z}
    chip = sp * RING + x

    def neighbour(dim, step):
        there = dict(at)
        there[dim] = mod4(at[dim] + step)
        return (there["z"] * RING + there["y"], there["x"] * 2 + c)

    def chip_at(step):
        other = lax.rem(chip + step + 64, 64)
        return (other // RING, lax.rem(other, RING) * 2 + c)

    peer = (sp, x * 2 + 1 - c)

    own_q = pltpu.make_async_copy(q_w, g_q.at[:, x, z, y], local_sem.at[0])
    own_o = pltpu.make_async_copy(o_w, g_o.at[:, x, z, y], local_sem.at[1])
    own_in = pltpu.make_async_copy(inputs.at[pl.ds(x * 2 * BLK, 2 * BLK)], staged, local_sem.at[2])
    own_q.start()
    own_o.start()
    own_in.start()

    barrier = pltpu.get_barrier_semaphore()
    greeted = [neighbour(d, s) for d in DIMS for s in (1, -1)] + [neighbour("x", 2), chip_at(1), chip_at(-1), peer]
    for device in greeted:
        pl.semaphore_signal(barrier, inc=1, device_id=device, device_id_type=MESH)

    for l in range(LAYERS):
        g_kv[l, x, z, y] = jnp.concatenate([k_w[l], v_w[l]], axis=1)
    own_q.wait()
    own_o.wait()
    pl.semaphore_wait(barrier, len(greeted))

    pending = []
    blocks = (g_q, g_kv, g_o)

    def view(stage, r, pos, half):
        phase, lo, hi = STAGES[stage]
        rotation = ROTATIONS[r]
        index = {d: at[d] for d in DIMS}
        index[rotation[phase]] = pos
        gathered = rotation[:phase]
        for d in gathered:
            index[d] = slice(None)
        rows = slice(None)
        if phase == 0:
            rows = slice(half * 64, half * 64 + 64)
        else:
            outer = [d for d in DIMS if d in gathered][0]
            index[outer] = slice(half * 2, half * 2 + 2)
        return blocks[r].at[(slice(lo, hi),) + tuple(index[d] for d in DIMS) + (rows,)]

    def copy_of(stage, r, pos, half, slot, device):
        k = (stage * 3 + r) * 6 + slot
        ref = view(stage, r, pos, half)
        return pltpu.make_async_remote_copy(
            src_ref=ref, dst_ref=ref, send_sem=send_sem.at[k], recv_sem=recv_sem.at[k],
            device_id=device, device_id_type=MESH,
        )

    def send(stage, r, back, half, slot, step):
        dim = ROTATIONS[r][STAGES[stage][0]]
        copy = copy_of(stage, r, mod4(at[dim] + back), half, slot, neighbour(dim, step))
        copy.start()
        pending.append(copy)

    def arrived(stage, r, back, half, slot):
        dim = ROTATIONS[r][STAGES[stage][0]]
        copy_of(stage, r, mod4(at[dim] + back), half, slot, peer).wait_recv()

    def first(stage):
        for r in range(3):
            send(stage, r, 0, 0, 0, 1)
            send(stage, r, 0, 1, 1, -1)

    def second(stage):
        for r in range(3):
            send(stage, r, 0, 1, 2, 1)
            send(stage, r, 0, 0, 3, -1)

    def forward(stage):
        for r in range(3):
            arrived(stage, r, -1, 0, 0)
            send(stage, r, -1, 0, 4, 1)
            arrived(stage, r, 1, 1, 1)
            send(stage, r, 1, 1, 5, -1)

    def finish(stage):
        for r in range(3):
            arrived(stage, r, -1, 1, 2)
            arrived(stage, r, 1, 0, 3)
            arrived(stage, r, 2, 0, 4)
            arrived(stage, r, 2, 1, 5)

    def sink_copy(i):
        return pltpu.make_async_remote_copy(
            src_ref=sink_tile, dst_ref=sinks.at[x], send_sem=sink_ssem.at[i - 1], recv_sem=sink_rsem.at[i - 1],
            device_id=neighbour("x", i), device_id_type=MESH,
        )

    def norm_into(src, first_row, rows, gain, write):
        def body(i, carry):
            at_row = pl.ds(pl.multiple_of(first_row + i * 16, 16), 16)
            v = src(i * 16, at_row)
            root = lax.rsqrt(jnp.mean(v * v, axis=-1, keepdims=True) + EPS)
            write(at_row, v * root * gain)
            return carry

        lax.fori_loop(0, rows // 16, body, 0)

    lane = lax.broadcasted_iota(jnp.int32, (2 * BLK, BLK), 1)
    low_half = lax.rem(lane, HEAD_DIM) < HEAD_DIM // 2
    low_head = lane < HEAD_DIM

    def turned(v, cos, sin):
        swapped = jnp.where(low_half, pltpu.roll(v, BLK - 32, 1), pltpu.roll(v, 32, 1))
        return v * cos[...] + swapped * sin[...]

    def project_kv(l):
        def body(i, carry):
            w = jnp.concatenate([g_kv[l, 2 * i + j].reshape(D, BLK) for j in range(2)], axis=1)
            raw = jnp.dot(normed[l], w, preferred_element_type=F32)
            for j in range(2):
                kv = turned(raw[:, j * BLK : (j + 1) * BLK], kv_cos, kv_sin)
                kv_rows[l, 2 * i + j, pl.ds(BLK, 2 * BLK)] = kv.astype(BF16)
            return carry

        lax.fori_loop(0, 2, body, 0)

    def project_q(l):
        def body(i, carry):
            w = jnp.concatenate([g_q[l, 2 * i + j].reshape(D, BLK) for j in range(2)], axis=1)
            raw = jnp.dot(normed[l], w, preferred_element_type=F32)
            for j in range(2):
                q = turned(raw[:, j * BLK : (j + 1) * BLK], q_cos, q_sin)
                head0 = jnp.where(low_head, q, 0.0).astype(BF16)
                head1 = jnp.where(low_head, pltpu.roll(q, HEAD_DIM, 1), 0.0).astype(BF16)
                for b in range(2):
                    q_rows[2 * i + j, b, pl.ds(0, BLK)] = head0[b * BLK : (b + 1) * BLK]
                    q_rows[2 * i + j, b, pl.ds(BLK, BLK)] = head1[b * BLK : (b + 1) * BLK]
            return carry

        lax.fori_loop(0, 2, body, 0)

    def halo(l):
        to_right = pltpu.make_async_remote_copy(
            src_ref=kv_rows.at[l, :, pl.ds(2 * BLK, BLK)], dst_ref=kv_rows.at[l, :, pl.ds(0, BLK)],
            send_sem=halo_send.at[l, 0], recv_sem=halo_recv.at[l, 0], device_id=chip_at(1), device_id_type=MESH,
        )
        to_left = pltpu.make_async_remote_copy(
            src_ref=kv_rows.at[l, :, pl.ds(BLK, BLK)], dst_ref=kv_rows.at[l, :, pl.ds(3 * BLK, BLK)],
            send_sem=halo_send.at[l, 1], recv_sem=halo_recv.at[l, 1], device_id=chip_at(-1), device_id_type=MESH,
        )
        return to_right, to_left

    low_lane = lax.broadcasted_iota(jnp.int32, (BLK, BLK), 1) < HEAD_DIM

    def attention(l, lo, hi):
        def body(i, carry):
            h, b = i // 2, lax.rem(i, 2)
            kv = kv_rows[l, h, pl.ds(pl.multiple_of(b * BLK, BLK), 3 * BLK)]
            s = lax.dot_general(q_rows[h, b], kv, (((1,), (1,)), ((), ())), preferred_element_type=F32)
            limits = bias[b]
            tops = []
            for g in range(2):
                own = s[g * BLK : (g + 1) * BLK] + limits
                sink = sinks[h, pl.ds(2 * l + g, 1), pl.ds(0, 1)]
                m = jnp.maximum(jnp.max(own, axis=1, keepdims=True), sink)
                p = jnp.exp(own - m)
                total = jnp.sum(p, axis=1, keepdims=True) + jnp.exp(sink - m)
                o = jnp.dot(p.astype(BF16), kv, preferred_element_type=F32)
                tops.append(o / total)
            both = jnp.where(low_lane, pltpu.roll(tops[0], HEAD_DIM, 1), tops[1])
            att[h, pl.ds(pl.multiple_of(b * BLK, BLK), BLK)] = both.astype(BF16)
            return carry

        lax.fori_loop(2 * lo, 2 * hi, body, 0)

    def project_out(l, block, dst):
        rows = pl.ds(pl.multiple_of(block * BLK, BLK), BLK)
        lhs = jnp.concatenate([att[h, rows] for h in range(RING)], axis=1)

        def body(i, carry):
            zz, yy = i // 2, lax.rem(i, 2) * 2
            w = jnp.concatenate([g_o[l, h, zz, pl.ds(yy, 2)].reshape(2 * BLK, BLK) for h in range(RING)], axis=1)
            r = lax.dot_general(lhs, w, (((1,), (1,)), ((), ())), preferred_element_type=F32)
            dst[:, pl.ds(pl.multiple_of(i * 2 * BLK, 2 * BLK), 2 * BLK)] = r
            return carry

        lax.fori_loop(0, 8, body, 0)

    def part_copy(l):
        return pltpu.make_async_remote_copy(
            src_ref=part_send.at[l], dst_ref=part_recv.at[l], send_sem=part_ssem.at[l], recv_sem=part_rsem.at[l],
            device_id=peer, device_id_type=MESH,
        )

    def norm_copy(l, block):
        rows = normed.at[l, pl.ds(pl.multiple_of(block * BLK, BLK), BLK)]
        return pltpu.make_async_remote_copy(
            src_ref=rows, dst_ref=rows, send_sem=norm_ssem.at[l], recv_sem=norm_rsem.at[l],
            device_id=peer, device_id_type=MESH,
        )

    def summed(l):
        def src(i, at_row):
            rows = pl.ds(pl.multiple_of(i, 16), 16)
            return (part_own[rows] + part_recv[l, rows]).astype(BF16).astype(F32)

        return src

    def layer(l, between_q, between_att, between_out, last):
        project_kv(l)
        copies = halo(l)
        for copy in copies:
            copy.start()
            pending.append(copy)
        project_q(l)
        between_q()
        for copy in copies:
            copy.wait_recv()
        attention(l, 0, 4)
        between_att()
        project_out(l, 1 - c, part_send.at[l])
        copy = part_copy(l)
        copy.start()
        pending.append(copy)
        project_out(l, c, part_own)
        between_out()
        copy.wait_recv()
        if last:
            gain = final_gain[...]

            def write(at_row, v):
                out[at_row] = v

            norm_into(summed(l), 0, BLK, gain, write)
            return
        gain = norm_gain[pl.ds(l + 1, 1)]

        def write(at_row, v):
            normed[l + 1, at_row] = v.astype(BF16)

        norm_into(summed(l), c * BLK, BLK, gain, write)
        copy = norm_copy(l + 1, c)
        copy.start()
        pending.append(copy)
        norm_copy(l + 1, 1 - c).wait_recv()

    first(0)
    second(0)
    for i in range(1, RING):
        copy = sink_copy(i)
        copy.start()
        pending.append(copy)
    sinks[x] = sink_tile[...]
    own_in.wait()

    def write_first(at_row, v):
        normed[0, at_row] = v.astype(BF16)

    norm_into(lambda i, at_row: staged[at_row].astype(F32), 0, BLK, norm_gain[pl.ds(0, 1)], write_first)
    forward(0)
    norm_into(lambda i, at_row: staged[at_row].astype(F32), BLK, BLK, norm_gain[pl.ds(0, 1)], write_first)
    finish(0)
    first(1)
    second(1)
    row_i = lax.broadcasted_iota(jnp.int32, (BLK, 3 * BLK), 0)
    col_j = lax.broadcasted_iota(jnp.int32, (BLK, 3 * BLK), 1)
    for b in range(2):
        position = (chip * 2 + b - 1) * BLK + col_j
        gap = col_j - row_i
        allowed = (gap >= 0) & (gap <= 2 * WINDOW) & (position >= 0) & (position < SEQ)
        bias[b] = jnp.where(allowed, 0.0, MASKED)
    forward(1)
    first(2)
    finish(1)
    first(3)
    second(2)
    second(3)
    forward(2)
    forward(3)
    for i in range(1, RING):
        pltpu.make_async_remote_copy(
            src_ref=sink_tile, dst_ref=sinks.at[mod4(x - i)], send_sem=sink_ssem.at[i - 1],
            recv_sem=sink_rsem.at[i - 1], device_id=peer, device_id_type=MESH,
        ).wait_recv()
    finish(2)
    first(4)
    finish(3)
    layer(0, lambda: second(4), lambda: forward(4), lambda: first(5), False)
    finish(4)
    layer(1, lambda: second(5), lambda: forward(5), lambda: None, False)
    finish(5)
    layer(2, lambda: None, lambda: None, lambda: None, True)
    for copy in pending:
        copy.wait_send()


def shards(inputs, norm_gain, query_weight, key_weight, value_weight, output_weight, sink_logit, final_gain):
    sp, tp = lax.axis_index("sp"), lax.axis_index("tp")
    chip = sp * RING + tp // 2
    half = HEAD_DIM // 2
    inverse = 10000.0 ** (-jnp.arange(half).astype(F32) / half)
    places = (chip * 2 * BLK + jnp.arange(2 * BLK, dtype=jnp.int32)).astype(F32)
    angles = places[:, None] * inverse[None, :]
    scale = float(D) ** (-0.5)
    cos, sin = jnp.cos(angles) * scale, jnp.sin(angles) * scale
    cos_head = jnp.concatenate([cos, cos], axis=1)
    sin_head = jnp.concatenate([-sin, sin], axis=1)
    one = jnp.ones_like(cos_head)
    q_cos = jnp.concatenate([cos_head, cos_head], axis=1) * 0.125
    q_sin = jnp.concatenate([sin_head, sin_head], axis=1) * 0.125
    kv_cos = jnp.concatenate([cos_head, one], axis=1)
    kv_sin = jnp.concatenate([sin_head, 0.0 * one], axis=1)
    sink_tile = jnp.pad(jnp.broadcast_to(sink_logit.reshape(2 * LAYERS, 1), (2 * LAYERS, BLK)), ((0, 2), (0, 0)))
    vmem = pl.BlockSpec(memory_space=pltpu.VMEM)
    anywhere = pl.BlockSpec(memory_space=pl.ANY)
    weights = pltpu.VMEM((LAYERS, RING, RING, RING, BLK, BLK), BF16)
    dma = pltpu.SemaphoreType.DMA
    return pl.pallas_call(
        kernel,
        out_shape=jax.ShapeDtypeStruct((BLK, D), F32),
        in_specs=[anywhere, anywhere, vmem, vmem, anywhere] + [vmem] * 7,
        out_specs=vmem,
        scratch_shapes=[
            weights, weights, weights,
            pltpu.VMEM((2 * BLK, D), BF16),
            pltpu.VMEM((LAYERS, 2 * BLK, D), BF16),
            pltpu.VMEM((LAYERS, RING, 4 * BLK, BLK), BF16),
            pltpu.VMEM((RING, 2, 2 * BLK, BLK), BF16),
            pltpu.VMEM((RING, 2 * BLK, BLK), BF16),
            pltpu.VMEM((BLK, D), F32),
            pltpu.VMEM((LAYERS, BLK, D), F32),
            pltpu.VMEM((LAYERS, BLK, D), F32),
            pltpu.VMEM((2, BLK, 3 * BLK), F32),
            pltpu.VMEM((RING, 8, BLK), F32),
            dma((N_IDS,)), dma((N_IDS,)), dma((3,)),
            dma((LAYERS, 2)), dma((LAYERS, 2)),
            dma((LAYERS,)), dma((LAYERS,)), dma((LAYERS,)), dma((LAYERS,)),
            dma((RING - 1,)), dma((RING - 1,)),
        ],
        compiler_params=pltpu.CompilerParams(
            collective_id=0, has_side_effects=True, vmem_limit_bytes=60 * 1024 * 1024
        ),
    )(
        inputs, query_weight, key_weight, value_weight, output_weight, norm_gain, final_gain.reshape(1, D),
        sink_tile, q_cos, q_sin, kv_cos, kv_sin,
    )


def solution(mesh):
    in_specs = (
        P("sp", None),
        P(),
        P(None, "sp", "tp"),
        P(None, "sp", "tp"),
        P(None, "sp", "tp"),
        P(None, "sp", "tp"),
        P(None, "tp"),
        P(),
    )
    out_specs = P(("sp", "tp"), None)
    return jax.shard_map(shards, mesh=mesh, in_specs=in_specs, out_specs=out_specs, check_vma=False)
```

```python
import math

import jax
import jax.numpy as jnp
from jax import lax
from jax.experimental import pallas as pl
from jax.experimental.pallas import tpu as pltpu
from jax.sharding import PartitionSpec as P

D = 2048
HEAD_DIM = 64
WINDOW = 128
LAYERS = 3
EPS = 1e-06
BLK = 128
RING = 4
SEQ = 16384
MASKED = -1e30
MESH = pl.DeviceIdType.MESH
F32 = jnp.float32
BF16 = jnp.bfloat16

ROTATIONS = (("x", "y", "z"), ("y", "z", "x"), ("z", "x", "y"))
DIMS = ("x", "z", "y")
KV, Q, O = 0, 1, 2
ROWS = (((0, 48), (48, 80), (80, 128)), ((0, 48), (48, 80), (80, 128)), ((0, 40), (40, 88), (88, 128)))
SPREADS = tuple((kind, lo, hi) for lo, hi in ((0, 1), (1, 3)) for kind in (KV, Q, O))
GROUPS = tuple((kind, layer) for layer in range(LAYERS) for kind in (KV, Q, O))
CHUNKS = 4
LOG2E = 1.4426950408889634


def mod4(v):
    return lax.rem(v + 2 * RING, RING)


def kernel(
    inputs, q_w, k_w, v_w, o_w, norm_gain_in, sink_in,
    out,
    norm_gain, sink_logit, w_all, staged, normed, kv_rows, q_rows, att, part_own, part_send, part_recv, bias, sinks,
    sink_tile, tables,
    spread_send, spread_recv, ring_send, ring_recv, local_sem, halo_send, halo_recv, part_ssem, part_rsem, sink_sem,
):
    sp, tp = lax.axis_index("sp"), lax.axis_index("tp")
    z, y = sp // RING, lax.rem(sp, RING)
    x, c = tp // 2, lax.rem(tp, 2)
    at = {"x": x, "y": y, "z": z}
    chip = sp * RING + x

    def neighbour(dim, step):
        there = dict(at)
        there[dim] = mod4(at[dim] + step)
        return (there["z"] * RING + there["y"], there["x"] * 2 + c)

    def chip_at(step):
        other = lax.rem(chip + step + 64, 64)
        return (other // RING, lax.rem(other, RING) * 2 + c)

    peer = (sp, x * 2 + 1 - c)

    def own_block(first, count):
        return w_all.at[:, x, z, y, pl.ds(first, count)]

    own = [
        pltpu.make_async_copy(k_w, own_block(0, HEAD_DIM), local_sem.at[0]),
        pltpu.make_async_copy(v_w, own_block(HEAD_DIM, HEAD_DIM), local_sem.at[1]),
        pltpu.make_async_copy(q_w, own_block(Q * BLK, BLK), local_sem.at[2]),
        pltpu.make_async_copy(o_w, own_block(O * BLK, BLK), local_sem.at[3]),
    ]
    small = [
        pltpu.make_async_copy(sink_in, sink_logit, local_sem.at[4]),
        pltpu.make_async_copy(norm_gain_in, norm_gain, local_sem.at[5]),
        pltpu.make_async_copy(inputs.at[pl.ds(x * 2 * BLK, 2 * BLK)], staged, local_sem.at[6]),
    ]
    for copy in own + small:
        copy.start()

    barrier = pltpu.get_barrier_semaphore()
    greeted = [neighbour(d, s) for d in DIMS for s in (1, 2, 3)] + [peer]
    for device in greeted:
        pl.semaphore_signal(barrier, inc=1, device_id=device, device_id_type=MESH)
    for copy in own:
        copy.wait()
    pl.semaphore_wait(barrier, len(greeted))

    unsent = []

    def remote(src, dst, ssem, rsem, device):
        return pltpu.make_async_remote_copy(
            src_ref=src, dst_ref=dst, send_sem=ssem, recv_sem=rsem, device_id=device, device_id_type=MESH
        )

    def all_in(ref, sem):
        remote(ref, ref, sem, sem, peer).wait_recv()

    def all_out(ref, sem):
        unsent.append(remote(ref, ref, sem, sem, peer))

    def some_blocks(kind, lo, hi, xs, zs, ys):
        return w_all.at[lo:hi, 0:xs, 0:zs, 0:ys, pl.ds(kind * BLK, BLK)]

    def view(kind, lo, hi, r, phase, pos, half):
        rotation = ROTATIONS[r]
        index = {d: at[d] for d in DIMS}
        index[rotation[phase]] = pos
        for d in rotation[:phase]:
            index[d] = slice(None)
        if half is not None:
            outer = [d for d in DIMS if d in rotation[:phase]][0]
            index[outer] = slice(half * 2, half * 2 + 2)
        first, last = ROWS[kind][r]
        rows = slice(kind * BLK + first, kind * BLK + last)
        return w_all.at[(slice(lo, hi),) + tuple(index[d] for d in DIMS) + (rows,)]

    def spread(i):
        kind, lo, hi = SPREADS[i]
        for r in range(3):
            dim = ROTATIONS[r][0]
            ref = view(kind, lo, hi, r, 0, at[dim], None)
            for step in (1, 3, 2):
                remote(ref, ref, spread_send.at[i], spread_recv.at[i], neighbour(dim, step)).start()
        all_out(some_blocks(kind, lo, hi, 3, 1, 1), spread_send.at[i])

    def spread_in(i):
        kind, lo, hi = SPREADS[i]
        all_in(some_blocks(kind, lo, hi, 3, 1, 1), spread_recv.at[i])

    def hop(group, phase, back, half, slot, step):
        kind, layer = GROUPS[group]
        for r in range(3):
            dim = ROTATIONS[r][phase]
            ref = view(kind, layer, layer + 1, r, phase, mod4(at[dim] + back), half)
            ssem, rsem = ring_send.at[2 * group + phase - 1], ring_recv.at[4 * group + slot]
            remote(ref, ref, ssem, rsem, neighbour(dim, step)).start()

    def landed(group, slot, xs, zs, ys):
        kind, layer = GROUPS[group]
        all_in(some_blocks(kind, layer, layer + 1, xs, zs, ys), ring_recv.at[4 * group + slot])

    def plane(g):
        hop(g, 1, 0, None, 0, 1)
        hop(g, 1, 0, None, 0, -1)

    def plane_on(g):
        landed(g, 0, 2, 1, 4)
        hop(g, 1, -1, 0, 1, 1)
        hop(g, 1, 1, 1, 1, -1)
        kind, layer = GROUPS[g]
        all_out(some_blocks(kind, layer, layer + 1, 3, 1, 4), ring_send.at[2 * g])

    def plane_in(g):
        landed(g, 1, 1, 1, 4)

    def cube(g):
        hop(g, 2, 0, 0, 2, 1)
        hop(g, 2, 0, 1, 2, -1)
        hop(g, 2, 0, 1, 3, 1)
        hop(g, 2, 0, 0, 3, -1)

    def cube_on(g):
        landed(g, 2, 1, 4, 4)
        hop(g, 2, -1, 0, 3, 1)
        hop(g, 2, 1, 1, 3, -1)
        kind, layer = GROUPS[g]
        all_out(some_blocks(kind, layer, layer + 1, 3, 4, 4), ring_send.at[2 * g + 1])

    def cube_in(g):
        landed(g, 3, 2, 4, 4)

    def norm_rows(src, rows, write):
        def body(i, carry):
            at_row = pl.ds(pl.multiple_of(i * 16, 16), 16)
            v = src(at_row)
            root = lax.rsqrt(jnp.mean(v * v, axis=-1, keepdims=True) + EPS)
            write(at_row, v * root)
            return carry

        lax.fori_loop(0, rows // 16, body, 0)

    lane = lax.broadcasted_iota(jnp.int32, (2 * BLK, BLK), 1)
    low_half = lax.rem(lane, HEAD_DIM) < HEAD_DIM // 2
    low_head = lane < HEAD_DIM

    def make_tables():
        row = lax.broadcasted_iota(jnp.int32, (2 * BLK, BLK), 0) + chip * 2 * BLK
        place = lax.rem(lane, HEAD_DIM // 2).astype(F32)
        angle = row.astype(F32) * jnp.exp(place * (-math.log(10000.0) * 2 / HEAD_DIM))
        scale = float(D) ** (-0.5)
        cos = jnp.cos(angle) * scale
        sin = jnp.where(low_half, -scale, scale) * jnp.sin(angle)
        tables[0] = cos * (0.125 * LOG2E)
        tables[1] = sin * (0.125 * LOG2E)
        tables[2] = jnp.where(low_head, cos, 1.0)
        tables[3] = jnp.where(low_head, sin, 0.0)

    def make_bias():
        row_i = lax.broadcasted_iota(jnp.int32, (BLK, 3 * BLK), 0)
        col_j = lax.broadcasted_iota(jnp.int32, (BLK, 3 * BLK), 1)
        gap = col_j - row_i
        for b in range(2):
            position = (chip * 2 + b - 1) * BLK + col_j
            allowed = (gap >= 0) & (gap <= 2 * WINDOW) & (position >= 0) & (position < SEQ)
            bias[b] = jnp.where(allowed, 0.0, MASKED)

    def turned(v, which):
        swapped = jnp.where(low_half, pltpu.roll(v, BLK - 32, 1), pltpu.roll(v, 32, 1))
        return v * tables[which] + swapped * tables[which + 1]

    def project_kv(l):
        def body(i, carry):
            w = jnp.concatenate(
                [
                    jnp.concatenate([w_all[l, 2 * i + j, n // RING, n % RING, pl.ds(0, BLK)] for n in range(16)], axis=1)
                    for j in range(2)
                ],
                axis=0,
            )
            raw = lax.dot_general(normed[l], w, (((1,), (1,)), ((), ())), preferred_element_type=F32)
            for j in range(2):
                kv = turned(raw[:, j * BLK : (j + 1) * BLK], 2)
                kv_rows[l, 2 * i + j, pl.ds(BLK, 2 * BLK)] = kv.astype(BF16)
            return carry

        lax.fori_loop(0, 2, body, 0)

    def project_q(l):
        def body(i, carry):
            w = jnp.concatenate(
                [w_all[l, 2 * i + j, :, :, pl.ds(Q * BLK, BLK)].reshape(D, BLK) for j in range(2)], axis=1
            )
            raw = jnp.dot(normed[l], w, preferred_element_type=F32)
            for j in range(2):
                q = turned(raw[:, j * BLK : (j + 1) * BLK], 0)
                head0 = jnp.where(low_head, q, 0.0).astype(BF16)
                head1 = jnp.where(low_head, pltpu.roll(q, HEAD_DIM, 1), 0.0).astype(BF16)
                for b in range(2):
                    q_rows[2 * i + j, b, pl.ds(0, BLK)] = head0[b * BLK : (b + 1) * BLK]
                    q_rows[2 * i + j, b, pl.ds(BLK, BLK)] = head1[b * BLK : (b + 1) * BLK]
            return carry

        lax.fori_loop(0, 2, body, 0)

    def halo(l):
        rows = kv_rows.at[l]
        low, high = pl.ds(BLK, BLK), pl.ds(2 * BLK, BLK)
        sems = halo_send.at[l], halo_recv.at[l]
        remote(rows.at[:, high], rows.at[:, pl.ds(0, BLK)], *sems, chip_at(1)).start()
        remote(rows.at[:, low], rows.at[:, pl.ds(3 * BLK, BLK)], *sems, chip_at(-1)).start()
        all_out(rows.at[:, pl.ds(0, 2 * BLK)], sems[0])

    def halo_in(l):
        all_in(kv_rows.at[l, :, pl.ds(0, 2 * BLK)], halo_recv.at[l])

    low_lane = lax.broadcasted_iota(jnp.int32, (BLK, BLK), 1) < HEAD_DIM
    low_key = lax.broadcasted_iota(jnp.int32, (3 * BLK, BLK), 1) < HEAD_DIM

    def attention(l, lo, hi):
        def body(h, carry):
            for b in range(2):
                kv = kv_rows[l, h, pl.ds(b * BLK, 3 * BLK)]
                ones_v = jnp.where(low_key, jnp.ones_like(kv), kv)
                s = lax.dot_general(q_rows[h, b], kv, (((1,), (1,)), ((), ())), preferred_element_type=F32)
                sums, extra = [], []
                for g in range(2):
                    mine = s[g * BLK : (g + 1) * BLK] + bias[b]
                    sink = sinks[h, pl.ds(2 * l + g, 1), pl.ds(0, 1)]
                    m = jnp.maximum(jnp.max(mine, axis=1, keepdims=True), sink)
                    p = jnp.exp2(mine - m).astype(BF16)
                    sums.append(jnp.dot(p, ones_v, preferred_element_type=F32))
                    extra.append(jnp.exp2(sink - m))
                top = jnp.where(low_lane, pltpu.roll(sums[0], HEAD_DIM, 1), sums[1])
                below = jnp.where(low_lane, sums[0], pltpu.roll(sums[1], HEAD_DIM, 1))
                below = below + jnp.where(low_lane, extra[0], extra[1])
                att[h, pl.ds(b * BLK, BLK)] = (top / below).astype(BF16)
            return carry

        lax.fori_loop(lo, hi, body, 0)

    def part_rows(l, block):
        return pl.ds(pl.multiple_of(block * BLK, BLK), BLK) if l == LAYERS - 1 else slice(None)

    def send_part(l, j):
        cols = pl.ds(j * (D // CHUNKS), D // CHUNKS)
        rows = part_rows(l, 1 - c)
        remote(
            part_send.at[l, rows, cols], part_recv.at[l, rows, cols], part_ssem.at[l], part_rsem.at[l], peer
        ).start()

    def project_out(l):
        lhs = jnp.concatenate([att[h] for h in range(RING)], axis=1)
        for j in range(CHUNKS):

            def body(i, carry):
                pair = pl.ds(lax.rem(i, 2) * 2, 2)
                w = jnp.concatenate(
                    [w_all[l, h, i // 2, pair, pl.ds(O * BLK, BLK)].reshape(2 * BLK, BLK) for h in range(RING)],
                    axis=1,
                )
                r = lax.dot_general(lhs, w, (((1,), (1,)), ((), ())), preferred_element_type=F32)
                cols = pl.ds(pl.multiple_of(i * 2 * BLK, 2 * BLK), 2 * BLK)
                part_own[:, cols] = r
                part_send[l, :, cols] = r.astype(BF16)
                return carry

            lax.fori_loop(2 * j, 2 * j + 2, body, 0)
            if j > 0:
                send_part(l, j - 1)

    def parts_in(l):
        all_in(part_recv.at[l, part_rows(l, c)], part_rsem.at[l])

    def layer(l, steps):
        project_kv(l)
        steps[0]()
        halo(l)
        steps[1]()
        project_q(l)
        halo_in(l)
        steps[2]()
        attention(l, 0, 2)
        steps[3]()
        attention(l, 2, 4)
        steps[4]()
        project_out(l)
        steps[5]()
        send_part(l, CHUNKS - 1)
        all_out(part_send.at[l, part_rows(l, 1 - c)], part_ssem.at[l])
        parts_in(l)
        if l == LAYERS - 1:
            mine = part_rows(l, c)
            out[...] = (part_own[mine] + part_recv[l, mine].astype(F32)).astype(BF16)
            return

        def state(at_row):
            return (part_own[at_row] + part_recv[l, at_row].astype(F32)).astype(BF16).astype(F32)

        gain = norm_gain[pl.ds(l + 1, 1)]

        def write_normed(at_row, v):
            normed[l + 1, at_row] = (v * gain).astype(BF16)

        norm_rows(state, 2 * BLK, write_normed)
        steps[6]()

    def visits(*steps):
        return [lambda calls=calls: [f(*a) for f, *a in calls] for calls in steps]

    for i in range(3):
        spread(i)
    for copy in small:
        copy.wait()
    for l in range(LAYERS):
        for g in range(2):
            sink_tile[pl.ds(2 * l + g, 1)] = jnp.broadcast_to(sink_logit[pl.ds(g, 1), pl.ds(l, 1)], (1, BLK)) * LOG2E
    sinks[x] = sink_tile[...]
    for g in range(3):
        spread_in(g)
        plane(g)
    for i in range(3, 6):
        spread(i)
    for i in range(1, RING):
        remote(sink_tile, sinks.at[x], sink_sem.at[0], sink_sem.at[1], neighbour("x", i)).start()
    all_out(sinks.at[0:3], sink_sem.at[0])
    gain = norm_gain[pl.ds(0, 1)]

    def write_first(at_row, v):
        normed[0, at_row] = (v * gain).astype(BF16)

    plane_on(0)
    plane_on(1)
    plane_in(0)
    cube(0)
    norm_rows(lambda at_row: staged[at_row].astype(F32), 2 * BLK, write_first)
    plane_on(2)
    spread_in(3)
    plane(3)
    plane_in(1)
    cube(1)
    make_bias()
    cube_on(0)
    spread_in(4)
    plane(4)
    plane_on(3)
    plane_in(2)
    cube(2)
    make_tables()
    spread_in(5)
    plane(5)
    plane_on(4)
    all_in(sinks.at[0:3], sink_sem.at[1])
    cube_in(0)
    last = len(GROUPS) - 1
    for l in range(LAYERS):
        g = 3 * l
        plan = (
            [],
            [(cube_on, 1), (plane_in, 3), (cube, 3), (cube_on, 2), (plane_on, 5), (plane, 6), (cube_in, 1)],
            [(plane_on, 6), (plane, 7), (plane_in, 4), (cube, 4)],
            [(cube_on, 3)],
            [(cube_in, 2)],
            [(plane_on, 7), (plane, 8), (plane_in, 5), (cube, 5)],
            [(cube_in, 3)],
        )
        layer(l, visits(*([(f, g + n) for f, n in step if g + n <= last] for step in plan)))
    for copy in unsent:
        copy.wait_send()


def last_norm(rows, gain, out):
    v = rows[...].astype(F32)
    out[...] = v * lax.rsqrt(jnp.mean(v * v, axis=-1, keepdims=True) + EPS) * gain[...]


def shards(inputs, norm_gain, query_weight, key_weight, value_weight, output_weight, sink_logit, final_gain):
    vmem = pl.BlockSpec(memory_space=pltpu.VMEM)
    hbm = pl.BlockSpec(memory_space=pltpu.HBM)
    dma = pltpu.SemaphoreType.DMA
    rows = pl.pallas_call(
        kernel,
        out_shape=jax.ShapeDtypeStruct((BLK, D), BF16),
        in_specs=[hbm] * 7,
        out_specs=vmem,
        scratch_shapes=[
            pltpu.VMEM((LAYERS, D), F32),
            pltpu.VMEM((2, LAYERS), F32),
            pltpu.VMEM((LAYERS, RING, RING, RING, 3 * BLK, BLK), BF16),
            pltpu.VMEM((2 * BLK, D), BF16),
            pltpu.VMEM((LAYERS, 2 * BLK, D), BF16),
            pltpu.VMEM((LAYERS, RING, 4 * BLK, BLK), BF16),
            pltpu.VMEM((RING, 2, 2 * BLK, BLK), BF16),
            pltpu.VMEM((RING, 2 * BLK, BLK), BF16),
            pltpu.VMEM((2 * BLK, D), F32),
            pltpu.VMEM((LAYERS, 2 * BLK, D), BF16),
            pltpu.VMEM((LAYERS, 2 * BLK, D), BF16),
            pltpu.VMEM((2, BLK, 3 * BLK), F32),
            pltpu.VMEM((RING, 8, BLK), F32),
            pltpu.VMEM((8, BLK), F32),
            pltpu.VMEM((4, 2 * BLK, BLK), F32),
            dma((len(SPREADS),)), dma((len(SPREADS),)), dma((2 * len(GROUPS),)), dma((4 * len(GROUPS),)),
            dma((7,)), dma((LAYERS,)), dma((LAYERS,)), dma((LAYERS,)), dma((LAYERS,)), dma((2,)),
        ],
        compiler_params=pltpu.CompilerParams(
            collective_id=0, has_side_effects=True, vmem_limit_bytes=67043328
        ),
    )(
        inputs, query_weight, jnp.swapaxes(key_weight, 1, 2), jnp.swapaxes(value_weight, 1, 2), output_weight,
        norm_gain, jnp.swapaxes(sink_logit, 0, 1),
    )
    step = BLK // 4
    return pl.pallas_call(
        last_norm,
        grid=(4,),
        out_shape=jax.ShapeDtypeStruct((BLK, D), F32),
        in_specs=[pl.BlockSpec((step, D), lambda i: (i, 0)), pl.BlockSpec((1, D), lambda i: (0, 0))],
        out_specs=pl.BlockSpec((step, D), lambda i: (i, 0)),
    )(rows, final_gain.reshape(1, D))


def solution(mesh):
    in_specs = (
        P("sp", None),
        P(),
        P(None, "sp", "tp"),
        P(None, "sp", "tp"),
        P(None, "sp", "tp"),
        P(None, "sp", "tp"),
        P(None, "tp"),
        P(),
    )
    out_specs = P(("sp", "tp"), None)
    return jax.shard_map(shards, mesh=mesh, in_specs=in_specs, out_specs=out_specs, check_vma=False)
```

```python
import math

import jax
import jax.numpy as jnp
from jax import lax
from jax.experimental import pallas as pl
from jax.experimental.pallas import tpu as pltpu
from jax.sharding import PartitionSpec as P

D = 2048
HEAD_DIM = 64
WINDOW = 128
LAYERS = 3
EPS = 1e-06
BLK = 128
RING = 4
SEQ = 16384
MASKED = -1e30
MESH = pl.DeviceIdType.MESH
F32 = jnp.float32
BF16 = jnp.bfloat16

ROTATIONS = (("x", "y", "z"), ("y", "z", "x"), ("z", "x", "y"))
DIMS = ("x", "z", "y")
KV, Q, O = 0, 1, 2
ROWS = (((0, 48), (48, 96), (96, 128)), ((0, 48), (48, 80), (80, 128)), ((0, 32), (32, 80), (80, 128)))
SPREADS = tuple((kind, lo, hi) for lo, hi in ((0, 1), (1, 3)) for kind in (KV, Q, O))
GROUPS = tuple((kind, layer) for layer in range(LAYERS) for kind in (KV, Q, O))
CHUNKS = 4
LOG2E = 1.4426950408889634


def mod4(v):
    return lax.rem(v + 2 * RING, RING)


def kernel(
    inputs, q_w, k_w, v_w, o_w, norm_gain_in, sink_in,
    out,
    norm_gain, sink_logit, w_all, staged, normed, kv_rows, q_rows, att, part_own, part_send, part_recv, bias, sinks,
    sink_tile, tables,
    spread_send, spread_recv, ring_send, ring_recv, local_sem, halo_send, halo_recv, part_ssem, part_rsem, sink_sem,
):
    sp, tp = lax.axis_index("sp"), lax.axis_index("tp")
    z, y = sp // RING, lax.rem(sp, RING)
    x, c = tp // 2, lax.rem(tp, 2)
    at = {"x": x, "y": y, "z": z}
    chip = sp * RING + x

    def neighbour(dim, step):
        there = dict(at)
        there[dim] = mod4(at[dim] + step)
        return (there["z"] * RING + there["y"], there["x"] * 2 + c)

    def chip_at(step):
        other = lax.rem(chip + step + 64, 64)
        return (other // RING, lax.rem(other, RING) * 2 + c)

    peer = (sp, x * 2 + 1 - c)

    def own_block(first, count):
        return w_all.at[:, x, z, y, pl.ds(first, count)]

    own = [
        pltpu.make_async_copy(k_w, own_block(0, HEAD_DIM), local_sem.at[0]),
        pltpu.make_async_copy(v_w, own_block(HEAD_DIM, HEAD_DIM), local_sem.at[1]),
        pltpu.make_async_copy(q_w, own_block(Q * BLK, BLK), local_sem.at[2]),
        pltpu.make_async_copy(o_w, own_block(O * BLK, BLK), local_sem.at[3]),
    ]
    small = [
        pltpu.make_async_copy(sink_in, sink_logit, local_sem.at[4]),
        pltpu.make_async_copy(norm_gain_in, norm_gain, local_sem.at[5]),
        pltpu.make_async_copy(inputs.at[pl.ds(x * 2 * BLK, 2 * BLK)], staged, local_sem.at[6]),
    ]
    for copy in own + small:
        copy.start()

    barrier = pltpu.get_barrier_semaphore()
    greeted = [neighbour(d, s) for d in DIMS for s in (1, 2, 3)] + [peer]
    for device in greeted:
        pl.semaphore_signal(barrier, inc=1, device_id=device, device_id_type=MESH)
    for copy in own:
        copy.wait()
    pl.semaphore_wait(barrier, len(greeted))

    unsent = []

    def remote(src, dst, ssem, rsem, device):
        return pltpu.make_async_remote_copy(
            src_ref=src, dst_ref=dst, send_sem=ssem, recv_sem=rsem, device_id=device, device_id_type=MESH
        )

    def all_in(ref, sem):
        remote(ref, ref, sem, sem, peer).wait_recv()

    def all_out(ref, sem):
        unsent.append(remote(ref, ref, sem, sem, peer))

    def some_blocks(kind, lo, hi, xs, zs, ys):
        return w_all.at[lo:hi, 0:xs, 0:zs, 0:ys, pl.ds(kind * BLK, BLK)]

    def view(kind, lo, hi, r, phase, pos, half):
        rotation = ROTATIONS[r]
        index = {d: at[d] for d in DIMS}
        index[rotation[phase]] = pos
        for d in rotation[:phase]:
            index[d] = slice(None)
        if half is not None:
            outer = [d for d in DIMS if d in rotation[:phase]][0]
            index[outer] = slice(half * 2, half * 2 + 2)
        first, last = ROWS[kind][r]
        rows = slice(kind * BLK + first, kind * BLK + last)
        return w_all.at[(slice(lo, hi),) + tuple(index[d] for d in DIMS) + (rows,)]

    def spread(i):
        kind, lo, hi = SPREADS[i]
        for r in range(3):
            dim = ROTATIONS[r][0]
            ref = view(kind, lo, hi, r, 0, at[dim], None)
            for step in (1, 3, 2):
                remote(ref, ref, spread_send.at[i], spread_recv.at[i], neighbour(dim, step)).start()
        all_out(some_blocks(kind, lo, hi, 3, 1, 1), spread_send.at[i])

    def spread_in(i):
        kind, lo, hi = SPREADS[i]
        all_in(some_blocks(kind, lo, hi, 3, 1, 1), spread_recv.at[i])

    def hop(group, phase, back, half, slot, step):
        kind, layer = GROUPS[group]
        for r in range(3):
            dim = ROTATIONS[r][phase]
            ref = view(kind, layer, layer + 1, r, phase, mod4(at[dim] + back), half)
            ssem, rsem = ring_send.at[2 * group + phase - 1], ring_recv.at[4 * group + slot]
            remote(ref, ref, ssem, rsem, neighbour(dim, step)).start()

    def landed(group, slot, xs, zs, ys):
        kind, layer = GROUPS[group]
        all_in(some_blocks(kind, layer, layer + 1, xs, zs, ys), ring_recv.at[4 * group + slot])

    def plane(g):
        hop(g, 1, 0, None, 0, 1)
        hop(g, 1, 0, None, 0, -1)

    def plane_on(g):
        landed(g, 0, 2, 1, 4)
        hop(g, 1, -1, 0, 1, 1)
        hop(g, 1, 1, 1, 1, -1)
        kind, layer = GROUPS[g]
        all_out(some_blocks(kind, layer, layer + 1, 3, 1, 4), ring_send.at[2 * g])

    def plane_in(g):
        landed(g, 1, 1, 1, 4)

    def cube(g):
        hop(g, 2, 0, 0, 2, 1)
        hop(g, 2, 0, 1, 2, -1)
        hop(g, 2, 0, 1, 3, 1)
        hop(g, 2, 0, 0, 3, -1)

    def cube_on(g):
        landed(g, 2, 1, 4, 4)
        hop(g, 2, -1, 0, 3, 1)
        hop(g, 2, 1, 1, 3, -1)
        kind, layer = GROUPS[g]
        all_out(some_blocks(kind, layer, layer + 1, 3, 4, 4), ring_send.at[2 * g + 1])

    def cube_in(g):
        landed(g, 3, 2, 4, 4)

    def norm_rows(src, first, rows, write):
        def body(i, carry):
            at_row = pl.ds(pl.multiple_of(first + i * 16, 16), 16)
            v = src(at_row)
            root = lax.rsqrt(jnp.mean(v * v, axis=-1, keepdims=True) + EPS)
            write(at_row, v * root)
            return carry

        lax.fori_loop(0, rows // 16, body, 0)

    lane = lax.broadcasted_iota(jnp.int32, (2 * BLK, BLK), 1)
    low_half = lax.rem(lane, HEAD_DIM) < HEAD_DIM // 2
    low_head = lane < HEAD_DIM

    def make_tables():
        row = lax.broadcasted_iota(jnp.int32, (2 * BLK, BLK), 0) + chip * 2 * BLK
        place = lax.rem(lane, HEAD_DIM // 2).astype(F32)
        angle = row.astype(F32) * jnp.exp(place * (-math.log(10000.0) * 2 / HEAD_DIM))
        scale = float(D) ** (-0.5)
        cos = jnp.cos(angle) * scale
        sin = jnp.where(low_half, -scale, scale) * jnp.sin(angle)
        tables[0] = cos * (0.125 * LOG2E)
        tables[1] = sin * (0.125 * LOG2E)
        tables[2] = jnp.where(low_head, cos, 1.0)
        tables[3] = jnp.where(low_head, sin, 0.0)

    def make_bias():
        row_i = lax.broadcasted_iota(jnp.int32, (BLK, 3 * BLK), 0)
        col_j = lax.broadcasted_iota(jnp.int32, (BLK, 3 * BLK), 1)
        gap = col_j - row_i
        for b in range(2):
            position = (chip * 2 + b - 1) * BLK + col_j
            allowed = (gap >= 0) & (gap <= 2 * WINDOW) & (position >= 0) & (position < SEQ)
            bias[b] = jnp.where(allowed, 0.0, MASKED)

    def turned(v, which):
        swapped = jnp.where(low_half, pltpu.roll(v, BLK - 32, 1), pltpu.roll(v, 32, 1))
        return v * tables[which] + swapped * tables[which + 1]

    def project_kv(l):
        def body(i, carry):
            w = jnp.concatenate(
                [
                    jnp.concatenate([w_all[l, 2 * i + j, n // RING, n % RING, pl.ds(0, BLK)] for n in range(16)], axis=1)
                    for j in range(2)
                ],
                axis=0,
            )
            raw = lax.dot_general(normed[l], w, (((1,), (1,)), ((), ())), preferred_element_type=F32)
            for j in range(2):
                kv = turned(raw[:, j * BLK : (j + 1) * BLK], 2)
                kv_rows[l, 2 * i + j, pl.ds(BLK, 2 * BLK)] = kv.astype(BF16)
            return carry

        lax.fori_loop(0, 2, body, 0)

    def project_q(l):
        def body(i, carry):
            w = jnp.concatenate(
                [w_all[l, 2 * i + j, :, :, pl.ds(Q * BLK, BLK)].reshape(D, BLK) for j in range(2)], axis=1
            )
            raw = jnp.dot(normed[l], w, preferred_element_type=F32)
            for j in range(2):
                q = turned(raw[:, j * BLK : (j + 1) * BLK], 0)
                head0 = jnp.where(low_head, q, 0.0).astype(BF16)
                head1 = jnp.where(low_head, pltpu.roll(q, HEAD_DIM, 1), 0.0).astype(BF16)
                for b in range(2):
                    q_rows[2 * i + j, b, pl.ds(0, BLK)] = head0[b * BLK : (b + 1) * BLK]
                    q_rows[2 * i + j, b, pl.ds(BLK, BLK)] = head1[b * BLK : (b + 1) * BLK]
            return carry

        lax.fori_loop(0, 2, body, 0)

    def halo(l):
        rows = kv_rows.at[l]
        low, high = pl.ds(BLK, BLK), pl.ds(2 * BLK, BLK)
        sems = halo_send.at[l], halo_recv.at[l]
        remote(rows.at[:, high], rows.at[:, pl.ds(0, BLK)], *sems, chip_at(1)).start()
        remote(rows.at[:, low], rows.at[:, pl.ds(3 * BLK, BLK)], *sems, chip_at(-1)).start()
        all_out(rows.at[:, pl.ds(0, 2 * BLK)], sems[0])

    def halo_in(l):
        all_in(kv_rows.at[l, :, pl.ds(0, 2 * BLK)], halo_recv.at[l])

    low_lane = lax.broadcasted_iota(jnp.int32, (BLK, BLK), 1) < HEAD_DIM
    low_key = lax.broadcasted_iota(jnp.int32, (3 * BLK, BLK), 1) < HEAD_DIM

    def attention(l, h):
        for b in range(2):
            kv = kv_rows[l, h, pl.ds(b * BLK, 3 * BLK)]
            ones_v = jnp.where(low_key, jnp.ones_like(kv), kv)
            s = lax.dot_general(q_rows[h, b], kv, (((1,), (1,)), ((), ())), preferred_element_type=F32)
            sums, extra = [], []
            for g in range(2):
                mine = s[g * BLK : (g + 1) * BLK] + bias[b]
                sink = sinks[h, pl.ds(2 * l + g, 1), pl.ds(0, 1)]
                m = jnp.maximum(jnp.max(mine, axis=1, keepdims=True), sink)
                p = jnp.exp2(mine - m).astype(BF16)
                sums.append(jnp.dot(p, ones_v, preferred_element_type=F32))
                extra.append(jnp.exp2(sink - m))
            top = jnp.where(low_lane, pltpu.roll(sums[0], HEAD_DIM, 1), sums[1])
            below = jnp.where(low_lane, sums[0], pltpu.roll(sums[1], HEAD_DIM, 1))
            below = below + jnp.where(low_lane, extra[0], extra[1])
            att[h, pl.ds(b * BLK, BLK)] = (top / below).astype(BF16)

    def part_rows(l, block):
        return pl.ds(pl.multiple_of(block * BLK, BLK), BLK) if l == LAYERS - 1 else slice(None)

    def send_part(l, j):
        cols = pl.ds(j * (D // CHUNKS), D // CHUNKS)
        rows = part_rows(l, 1 - c)
        remote(
            part_send.at[l, rows, cols], part_recv.at[l, rows, cols], part_ssem.at[l], part_rsem.at[l], peer
        ).start()

    def project_out(l, j):
        lhs = jnp.concatenate([att[h] for h in range(RING)], axis=1)

        def body(i, carry):
            pair = pl.ds(lax.rem(i, 2) * 2, 2)
            w = jnp.concatenate(
                [w_all[l, h, i // 2, pair, pl.ds(O * BLK, BLK)].reshape(2 * BLK, BLK) for h in range(RING)],
                axis=1,
            )
            r = lax.dot_general(lhs, w, (((1,), (1,)), ((), ())), preferred_element_type=F32)
            cols = pl.ds(pl.multiple_of(i * 2 * BLK, 2 * BLK), 2 * BLK)
            part_own[:, cols] = r
            part_send[l, :, cols] = r.astype(BF16)
            return carry

        lax.fori_loop(2 * j, 2 * j + 2, body, 0)
        if j > 0:
            send_part(l, j - 1)

    def parts_in(l):
        all_in(part_recv.at[l, part_rows(l, c)], part_rsem.at[l])

    def exchange(l):
        send_part(l, CHUNKS - 1)
        all_out(part_send.at[l, part_rows(l, 1 - c)], part_ssem.at[l])
        parts_in(l)
        if l == LAYERS - 1:
            mine = part_rows(l, c)
            out[...] = (part_own[mine] + part_recv[l, mine].astype(F32)).astype(BF16)

    def norm_half(l, half):
        gain = norm_gain[pl.ds(l + 1, 1)]

        def state(at_row):
            return (part_own[at_row] + part_recv[l, at_row].astype(F32)).astype(BF16).astype(F32)

        def write_normed(at_row, v):
            normed[l + 1, at_row] = (v * gain).astype(BF16)

        norm_rows(state, half * BLK, BLK, write_normed)

    def first_norm(half):
        gain = norm_gain[pl.ds(0, 1)]

        def write_first(at_row, v):
            normed[0, at_row] = (v * gain).astype(BF16)

        norm_rows(lambda at_row: staged[at_row].astype(F32), half * BLK, BLK, write_first)

    def share_sinks():
        for copy in small:
            copy.wait()
        for l in range(LAYERS):
            for g in range(2):
                sink = jnp.broadcast_to(sink_logit[pl.ds(g, 1), pl.ds(l, 1)], (1, BLK))
                sink_tile[pl.ds(2 * l + g, 1)] = sink * LOG2E
        sinks[x] = sink_tile[...]
        for i in range(1, RING):
            remote(sink_tile, sinks.at[x], sink_sem.at[0], sink_sem.at[1], neighbour("x", i)).start()
        all_out(sinks.at[0:3], sink_sem.at[0])

    def sinks_in():
        all_in(sinks.at[0:3], sink_sem.at[1])

    order = (
        (spread, 0), (spread, 2), (spread, 5), (make_tables,), (spread, 4), (spread, 1), (share_sinks,),
        (spread_in, 0), (plane, 0), (spread, 3), (spread_in, 2), (spread_in, 5), (plane, 5), (spread_in, 4),
        (make_bias,), (plane, 4), (plane_on, 0), (plane, 2), (spread_in, 1), (plane, 1), (first_norm, 0),
        (spread_in, 3), (plane_on, 5), (plane, 3), (plane_in, 0), (plane_on, 4), (plane_on, 2), (cube, 0),
        (plane_on, 1), (plane_on, 3), (first_norm, 1), (plane, 6), (plane_in, 2), (cube_on, 0), (cube, 2),
        (plane_in, 1), (plane_in, 5), (cube_in, 0), (cube, 1), (plane_in, 4), (project_kv, 0), (halo, 0),
        (cube_on, 1), (plane_in, 3), (cube_on, 2), (plane, 8), (cube, 3), (cube_in, 1), (plane_on, 6),
        (cube, 4), (sinks_in,), (halo_in, 0), (project_q, 0), (attention, 0, 0), (attention, 0, 1),
        (cube_on, 3), (attention, 0, 2), (attention, 0, 3), (cube_in, 2), (project_out, 0, 0),
        (project_out, 0, 1), (cube_on, 4), (project_out, 0, 2), (cube, 5), (plane, 7), (project_out, 0, 3),
        (exchange, 0), (plane_in, 6), (norm_half, 0, 0), (norm_half, 0, 1), (cube_in, 3), (project_kv, 1),
        (cube_in, 4), (halo, 1), (plane_on, 7), (cube_on, 5), (project_q, 1), (cube, 6), (halo_in, 1),
        (plane_on, 8), (attention, 1, 0), (plane_in, 7), (attention, 1, 1), (cube_on, 6), (attention, 1, 2),
        (cube_in, 5), (cube, 7), (attention, 1, 3), (project_out, 1, 0), (project_out, 1, 1),
        (project_out, 1, 2), (project_out, 1, 3), (exchange, 1), (cube_in, 6), (plane_in, 8),
        (norm_half, 1, 0), (cube_on, 7), (norm_half, 1, 1), (project_kv, 2), (halo, 2), (cube, 8),
        (cube_in, 7), (project_q, 2), (cube_on, 8), (halo_in, 2), (attention, 2, 0), (attention, 2, 1),
        (attention, 2, 2), (attention, 2, 3), (cube_in, 8), (project_out, 2, 0), (project_out, 2, 1),
        (project_out, 2, 2), (project_out, 2, 3), (exchange, 2),
    )
    for step, *arguments in order:
        step(*arguments)
    for copy in unsent:
        copy.wait_send()


def last_norm(rows, gain, out):
    v = rows[...].astype(F32)
    out[...] = v * lax.rsqrt(jnp.mean(v * v, axis=-1, keepdims=True) + EPS) * gain[...]


def shards(inputs, norm_gain, query_weight, key_weight, value_weight, output_weight, sink_logit, final_gain):
    vmem = pl.BlockSpec(memory_space=pltpu.VMEM)
    hbm = pl.BlockSpec(memory_space=pltpu.HBM)
    dma = pltpu.SemaphoreType.DMA
    rows = pl.pallas_call(
        kernel,
        out_shape=jax.ShapeDtypeStruct((BLK, D), BF16),
        in_specs=[hbm] * 7,
        out_specs=vmem,
        scratch_shapes=[
            pltpu.VMEM((LAYERS, D), F32),
            pltpu.VMEM((2, LAYERS), F32),
            pltpu.VMEM((LAYERS, RING, RING, RING, 3 * BLK, BLK), BF16),
            pltpu.VMEM((2 * BLK, D), BF16),
            pltpu.VMEM((LAYERS, 2 * BLK, D), BF16),
            pltpu.VMEM((LAYERS, RING, 4 * BLK, BLK), BF16),
            pltpu.VMEM((RING, 2, 2 * BLK, BLK), BF16),
            pltpu.VMEM((RING, 2 * BLK, BLK), BF16),
            pltpu.VMEM((2 * BLK, D), F32),
            pltpu.VMEM((LAYERS, 2 * BLK, D), BF16),
            pltpu.VMEM((LAYERS, 2 * BLK, D), BF16),
            pltpu.VMEM((2, BLK, 3 * BLK), F32),
            pltpu.VMEM((RING, 8, BLK), F32),
            pltpu.VMEM((8, BLK), F32),
            pltpu.VMEM((4, 2 * BLK, BLK), F32),
            dma((len(SPREADS),)), dma((len(SPREADS),)), dma((2 * len(GROUPS),)), dma((4 * len(GROUPS),)),
            dma((7,)), dma((LAYERS,)), dma((LAYERS,)), dma((LAYERS,)), dma((LAYERS,)), dma((2,)),
        ],
        compiler_params=pltpu.CompilerParams(
            collective_id=0, has_side_effects=True, vmem_limit_bytes=67043328
        ),
    )(
        inputs, query_weight, jnp.swapaxes(key_weight, 1, 2), jnp.swapaxes(value_weight, 1, 2), output_weight,
        norm_gain, jnp.swapaxes(sink_logit, 0, 1),
    )
    step = BLK // 4
    return pl.pallas_call(
        last_norm,
        grid=(4,),
        out_shape=jax.ShapeDtypeStruct((BLK, D), F32),
        in_specs=[pl.BlockSpec((step, D), lambda i: (i, 0)), pl.BlockSpec((1, D), lambda i: (0, 0))],
        out_specs=pl.BlockSpec((step, D), lambda i: (i, 0)),
    )(rows, final_gain.reshape(1, D))


def solution(mesh):
    in_specs = (
        P("sp", None),
        P(),
        P(None, "sp", "tp"),
        P(None, "sp", "tp"),
        P(None, "sp", "tp"),
        P(None, "sp", "tp"),
        P(None, "tp"),
        P(),
    )
    out_specs = P(("sp", "tp"), None)
    return jax.shard_map(shards, mesh=mesh, in_specs=in_specs, out_specs=out_specs, check_vma=False)
```

```python
import math

import jax
import jax.numpy as jnp
from jax import lax
from jax.experimental import pallas as pl
from jax.experimental.pallas import tpu as pltpu
from jax.sharding import PartitionSpec as P

D = 2048
HEAD_DIM = 64
WINDOW = 128
LAYERS = 3
EPS = 1e-06
BLK = 128
RING = 4
SEQ = 16384
MASKED = -1e30
MESH = pl.DeviceIdType.MESH
F32 = jnp.float32
BF16 = jnp.bfloat16

ROTATIONS = (("x", "y", "z"), ("y", "z", "x"), ("z", "x", "y"))
DIMS = ("x", "z", "y")
KV, Q, O = 0, 1, 2
ROWS = (((0, 48), (48, 96), (96, 128)), ((0, 48), (48, 80), (80, 128)), ((0, 32), (32, 80), (80, 128)))
SPREADS = tuple((kind, lo, hi) for lo, hi in ((0, 1), (1, 3)) for kind in (KV, Q, O))
GROUPS = tuple((kind, layer) for layer in range(LAYERS) for kind in (KV, Q, O))
CHUNKS = 4
LOG2E = 1.4426950408889634


def mod4(v):
    return lax.rem(v + 2 * RING, RING)


def kernel(
    inputs, q_w, k_w, v_w, o_w, norm_gain_in, sink_in,
    out,
    norm_gain, sink_logit, w_all, staged, normed, kv_rows, q_rows, att, part_own, part_send, part_recv, bias, sinks,
    sink_tile, tables,
    spread_send, spread_recv, ring_send, ring_recv, local_sem, halo_send, halo_recv, part_ssem, part_rsem, sink_sem,
):
    sp, tp = lax.axis_index("sp"), lax.axis_index("tp")
    z, y = sp // RING, lax.rem(sp, RING)
    x, c = tp // 2, lax.rem(tp, 2)
    at = {"x": x, "y": y, "z": z}
    chip = sp * RING + x

    def neighbour(dim, step):
        there = dict(at)
        there[dim] = mod4(at[dim] + step)
        return (there["z"] * RING + there["y"], there["x"] * 2 + c)

    def chip_at(step):
        other = lax.rem(chip + step + 64, 64)
        return (other // RING, lax.rem(other, RING) * 2 + c)

    peer = (sp, x * 2 + 1 - c)

    def own_block(first, count):
        return w_all.at[:, x, z, y, pl.ds(first, count)]

    own = [
        pltpu.make_async_copy(k_w, own_block(0, HEAD_DIM), local_sem.at[0]),
        pltpu.make_async_copy(v_w, own_block(HEAD_DIM, HEAD_DIM), local_sem.at[1]),
        pltpu.make_async_copy(q_w, own_block(Q * BLK, BLK), local_sem.at[2]),
        pltpu.make_async_copy(o_w, own_block(O * BLK, BLK), local_sem.at[3]),
    ]
    small = [
        pltpu.make_async_copy(sink_in, sink_logit, local_sem.at[4]),
        pltpu.make_async_copy(norm_gain_in, norm_gain, local_sem.at[5]),
        pltpu.make_async_copy(inputs.at[pl.ds(x * 2 * BLK, 2 * BLK)], staged, local_sem.at[6]),
    ]
    for copy in own + small:
        copy.start()

    barrier = pltpu.get_barrier_semaphore()
    greeted = [neighbour(d, s) for d in DIMS for s in (1, 2, 3)] + [peer]
    for device in greeted:
        pl.semaphore_signal(barrier, inc=1, device_id=device, device_id_type=MESH)
    for copy in own:
        copy.wait()
    pl.semaphore_wait(barrier, len(greeted))

    unsent = []

    def remote(src, dst, ssem, rsem, device):
        return pltpu.make_async_remote_copy(
            src_ref=src, dst_ref=dst, send_sem=ssem, recv_sem=rsem, device_id=device, device_id_type=MESH
        )

    def all_in(ref, sem):
        remote(ref, ref, sem, sem, peer).wait_recv()

    def all_out(ref, sem):
        unsent.append(remote(ref, ref, sem, sem, peer))

    def some_blocks(kind, lo, hi, xs, zs, ys):
        return w_all.at[lo:hi, 0:xs, 0:zs, 0:ys, pl.ds(kind * BLK, BLK)]

    def view(kind, lo, hi, r, phase, pos, half):
        rotation = ROTATIONS[r]
        index = {d: at[d] for d in DIMS}
        index[rotation[phase]] = pos
        for d in rotation[:phase]:
            index[d] = slice(None)
        if half is not None:
            outer = [d for d in DIMS if d in rotation[:phase]][0]
            index[outer] = slice(half * 2, half * 2 + 2)
        first, last = ROWS[kind][r]
        rows = slice(kind * BLK + first, kind * BLK + last)
        return w_all.at[(slice(lo, hi),) + tuple(index[d] for d in DIMS) + (rows,)]

    def spread(i):
        kind, lo, hi = SPREADS[i]
        for r in range(3):
            dim = ROTATIONS[r][0]
            ref = view(kind, lo, hi, r, 0, at[dim], None)
            for step in (1, 3, 2):
                remote(ref, ref, spread_send.at[i], spread_recv.at[i], neighbour(dim, step)).start()
        all_out(some_blocks(kind, lo, hi, 3, 1, 1), spread_send.at[i])

    def spread_in(i):
        kind, lo, hi = SPREADS[i]
        all_in(some_blocks(kind, lo, hi, 3, 1, 1), spread_recv.at[i])

    def hop(group, phase, back, half, slot, step):
        kind, layer = GROUPS[group]
        for r in range(3):
            dim = ROTATIONS[r][phase]
            ref = view(kind, layer, layer + 1, r, phase, mod4(at[dim] + back), half)
            ssem, rsem = ring_send.at[2 * group + phase - 1], ring_recv.at[4 * group + slot]
            remote(ref, ref, ssem, rsem, neighbour(dim, step)).start()

    def landed(group, slot, xs, zs, ys):
        kind, layer = GROUPS[group]
        all_in(some_blocks(kind, layer, layer + 1, xs, zs, ys), ring_recv.at[4 * group + slot])

    def plane(g):
        hop(g, 1, 0, None, 0, 1)
        hop(g, 1, 0, None, 0, -1)

    def plane_on(g):
        landed(g, 0, 2, 1, 4)
        hop(g, 1, -1, 0, 1, 1)
        hop(g, 1, 1, 1, 1, -1)
        kind, layer = GROUPS[g]
        all_out(some_blocks(kind, layer, layer + 1, 3, 1, 4), ring_send.at[2 * g])

    def plane_in(g):
        landed(g, 1, 1, 1, 4)

    def cube(g):
        hop(g, 2, 0, 0, 2, 1)
        hop(g, 2, 0, 1, 2, -1)

    def cube_more(g):
        hop(g, 2, 0, 1, 3, 1)
        hop(g, 2, 0, 0, 3, -1)

    def cube_on(g):
        landed(g, 2, 1, 4, 4)
        hop(g, 2, -1, 0, 3, 1)
        hop(g, 2, 1, 1, 3, -1)
        kind, layer = GROUPS[g]
        all_out(some_blocks(kind, layer, layer + 1, 3, 4, 4), ring_send.at[2 * g + 1])

    def cube_in(g):
        landed(g, 3, 2, 4, 4)

    def norm_rows(src, first, rows, write):
        def body(i, carry):
            at_row = pl.ds(pl.multiple_of(first + i * 16, 16), 16)
            v = src(at_row)
            root = lax.rsqrt(jnp.mean(v * v, axis=-1, keepdims=True) + EPS)
            write(at_row, v * root)
            return carry

        lax.fori_loop(0, rows // 16, body, 0)

    lane = lax.broadcasted_iota(jnp.int32, (2 * BLK, BLK), 1)
    low_half = lax.rem(lane, HEAD_DIM) < HEAD_DIM // 2
    low_head = lane < HEAD_DIM

    def make_tables():
        row = lax.broadcasted_iota(jnp.int32, (2 * BLK, BLK), 0) + chip * 2 * BLK
        place = lax.rem(lane, HEAD_DIM // 2).astype(F32)
        angle = row.astype(F32) * jnp.exp(place * (-math.log(10000.0) * 2 / HEAD_DIM))
        scale = float(D) ** (-0.5)
        cos = jnp.cos(angle) * scale
        sin = jnp.where(low_half, -scale, scale) * jnp.sin(angle)
        tables[0] = cos * (0.125 * LOG2E)
        tables[1] = sin * (0.125 * LOG2E)
        tables[2] = jnp.where(low_head, cos, 1.0)
        tables[3] = jnp.where(low_head, sin, 0.0)

    def make_bias():
        row_i = lax.broadcasted_iota(jnp.int32, (BLK, 3 * BLK), 0)
        col_j = lax.broadcasted_iota(jnp.int32, (BLK, 3 * BLK), 1)
        gap = col_j - row_i
        for b in range(2):
            position = (chip * 2 + b - 1) * BLK + col_j
            allowed = (gap >= 0) & (gap <= 2 * WINDOW) & (position >= 0) & (position < SEQ)
            bias[b] = jnp.where(allowed, 0.0, MASKED)

    def turned(v, which):
        swapped = jnp.where(low_half, pltpu.roll(v, BLK - 32, 1), pltpu.roll(v, 32, 1))
        return v * tables[which] + swapped * tables[which + 1]

    def project_kv(l):
        def body(i, carry):
            w = jnp.concatenate(
                [
                    jnp.concatenate([w_all[l, 2 * i + j, n // RING, n % RING, pl.ds(0, BLK)] for n in range(16)], axis=1)
                    for j in range(2)
                ],
                axis=0,
            )
            raw = lax.dot_general(normed[l], w, (((1,), (1,)), ((), ())), preferred_element_type=F32)
            for j in range(2):
                kv = turned(raw[:, j * BLK : (j + 1) * BLK], 2)
                kv_rows[l, 2 * i + j, pl.ds(BLK, 2 * BLK)] = kv.astype(BF16)
            return carry

        lax.fori_loop(0, 2, body, 0)

    def project_q(l):
        def body(i, carry):
            w = jnp.concatenate(
                [w_all[l, 2 * i + j, :, :, pl.ds(Q * BLK, BLK)].reshape(D, BLK) for j in range(2)], axis=1
            )
            raw = jnp.dot(normed[l], w, preferred_element_type=F32)
            for j in range(2):
                q = turned(raw[:, j * BLK : (j + 1) * BLK], 0)
                head0 = jnp.where(low_head, q, 0.0).astype(BF16)
                head1 = jnp.where(low_head, pltpu.roll(q, HEAD_DIM, 1), 0.0).astype(BF16)
                for b in range(2):
                    q_rows[2 * i + j, b, pl.ds(0, BLK)] = head0[b * BLK : (b + 1) * BLK]
                    q_rows[2 * i + j, b, pl.ds(BLK, BLK)] = head1[b * BLK : (b + 1) * BLK]
            return carry

        lax.fori_loop(0, 2, body, 0)

    def halo(l):
        rows = kv_rows.at[l]
        low, high = pl.ds(BLK, BLK), pl.ds(2 * BLK, BLK)
        sems = halo_send.at[l], halo_recv.at[l]
        remote(rows.at[:, high], rows.at[:, pl.ds(0, BLK)], *sems, chip_at(1)).start()
        remote(rows.at[:, low], rows.at[:, pl.ds(3 * BLK, BLK)], *sems, chip_at(-1)).start()
        all_out(rows.at[:, pl.ds(0, 2 * BLK)], sems[0])

    def halo_in(l):
        all_in(kv_rows.at[l, :, pl.ds(0, 2 * BLK)], halo_recv.at[l])

    low_lane = lax.broadcasted_iota(jnp.int32, (BLK, BLK), 1) < HEAD_DIM
    low_key = lax.broadcasted_iota(jnp.int32, (3 * BLK, BLK), 1) < HEAD_DIM

    def attention(l, h):
        for b in range(2):
            kv = kv_rows[l, h, pl.ds(b * BLK, 3 * BLK)]
            ones_v = jnp.where(low_key, jnp.ones_like(kv), kv)
            s = lax.dot_general(q_rows[h, b], kv, (((1,), (1,)), ((), ())), preferred_element_type=F32)
            sums, extra = [], []
            for g in range(2):
                mine = s[g * BLK : (g + 1) * BLK] + bias[b]
                sink = sinks[h, pl.ds(2 * l + g, 1), pl.ds(0, 1)]
                m = jnp.maximum(jnp.max(mine, axis=1, keepdims=True), sink)
                p = jnp.exp2(mine - m).astype(BF16)
                sums.append(jnp.dot(p, ones_v, preferred_element_type=F32))
                extra.append(jnp.exp2(sink - m))
            top = jnp.where(low_lane, pltpu.roll(sums[0], HEAD_DIM, 1), sums[1])
            below = jnp.where(low_lane, sums[0], pltpu.roll(sums[1], HEAD_DIM, 1))
            below = below + jnp.where(low_lane, extra[0], extra[1])
            att[h, pl.ds(b * BLK, BLK)] = (top / below).astype(BF16)

    def part_rows(l, block):
        return pl.ds(pl.multiple_of(block * BLK, BLK), BLK) if l == LAYERS - 1 else slice(None)

    def send_part(l, j):
        cols = pl.ds(j * (D // CHUNKS), D // CHUNKS)
        rows = part_rows(l, 1 - c)
        remote(
            part_send.at[l, rows, cols], part_recv.at[l, rows, cols], part_ssem.at[l], part_rsem.at[l], peer
        ).start()

    def project_out(l, j):
        lhs = jnp.concatenate([att[h] for h in range(RING)], axis=1)

        def body(i, carry):
            pair = pl.ds(lax.rem(i, 2) * 2, 2)
            w = jnp.concatenate(
                [w_all[l, h, i // 2, pair, pl.ds(O * BLK, BLK)].reshape(2 * BLK, BLK) for h in range(RING)],
                axis=1,
            )
            r = lax.dot_general(lhs, w, (((1,), (1,)), ((), ())), preferred_element_type=F32)
            cols = pl.ds(pl.multiple_of(i * 2 * BLK, 2 * BLK), 2 * BLK)
            part_own[:, cols] = r
            part_send[l, :, cols] = r.astype(BF16)
            return carry

        lax.fori_loop(2 * j, 2 * j + 2, body, 0)
        if j > 0:
            send_part(l, j - 1)

    def parts_in(l):
        all_in(part_recv.at[l, part_rows(l, c)], part_rsem.at[l])

    def exchange(l):
        send_part(l, CHUNKS - 1)
        all_out(part_send.at[l, part_rows(l, 1 - c)], part_ssem.at[l])
        parts_in(l)
        if l == LAYERS - 1:
            mine = part_rows(l, c)
            out[...] = (part_own[mine] + part_recv[l, mine].astype(F32)).astype(BF16)

    def norm_half(l, half):
        gain = norm_gain[pl.ds(l + 1, 1)]

        def state(at_row):
            return (part_own[at_row] + part_recv[l, at_row].astype(F32)).astype(BF16).astype(F32)

        def write_normed(at_row, v):
            normed[l + 1, at_row] = (v * gain).astype(BF16)

        norm_rows(state, half * BLK, BLK, write_normed)

    def first_norm(half):
        gain = norm_gain[pl.ds(0, 1)]

        def write_first(at_row, v):
            normed[0, at_row] = (v * gain).astype(BF16)

        norm_rows(lambda at_row: staged[at_row].astype(F32), half * BLK, BLK, write_first)

    def share_sinks():
        for copy in small:
            copy.wait()
        for l in range(LAYERS):
            for g in range(2):
                sink = jnp.broadcast_to(sink_logit[pl.ds(g, 1), pl.ds(l, 1)], (1, BLK))
                sink_tile[pl.ds(2 * l + g, 1)] = sink * LOG2E
        sinks[x] = sink_tile[...]
        for i in range(1, RING):
            remote(sink_tile, sinks.at[x], sink_sem.at[0], sink_sem.at[1], neighbour("x", i)).start()
        all_out(sinks.at[0:3], sink_sem.at[0])

    def sinks_in():
        all_in(sinks.at[0:3], sink_sem.at[1])

    order = (
        (spread, 1), (spread, 0), (make_bias,), (spread, 2), (spread, 3), (share_sinks,), (first_norm, 0),
        (spread, 5), (spread, 4), (spread_in, 1), (plane, 1), (spread_in, 2), (plane, 2), (spread_in, 0),
        (spread_in, 3), (plane, 0), (spread_in, 5), (plane, 3), (plane, 6), (plane, 5), (plane_on, 0),
        (spread_in, 4), (plane, 4), (make_tables,), (plane_on, 1), (plane, 8), (plane_on, 3), (plane_on, 2),
        (plane_in, 0), (cube, 0), (cube_more, 0), (plane_on, 6), (plane_on, 8), (first_norm, 1), (plane_on, 4),
        (plane_in, 1), (plane_in, 2), (plane_on, 5), (cube_on, 0), (cube, 1), (cube, 2), (cube_more, 1),
        (plane_in, 5), (plane_in, 3), (cube_in, 0), (project_kv, 0), (halo, 0), (cube_on, 1), (cube, 3),
        (cube_more, 2), (cube_on, 2), (plane_in, 4), (cube_in, 1), (cube, 4), (cube_more, 3), (project_q, 0),
        (cube_on, 3), (sinks_in,), (halo_in, 0), (cube_more, 4), (plane, 7), (cube, 5), (attention, 0, 0),
        (attention, 0, 1), (attention, 0, 2), (cube_in, 2), (attention, 0, 3), (project_out, 0, 0),
        (project_out, 0, 1), (project_out, 0, 2), (project_out, 0, 3), (plane_in, 8), (cube_on, 4),
        (exchange, 0), (plane_in, 6), (norm_half, 0, 0), (norm_half, 0, 1), (cube_in, 3), (project_kv, 1),
        (halo, 1), (plane_on, 7), (cube, 6), (cube_more, 5), (cube_on, 5), (plane_in, 7), (cube, 7),
        (cube_in, 4), (project_q, 1), (halo_in, 1), (cube_more, 6), (attention, 1, 0), (cube_on, 6),
        (attention, 1, 1), (attention, 1, 2), (cube_more, 7), (cube_in, 5), (attention, 1, 3), (cube_on, 7),
        (project_out, 1, 0), (project_out, 1, 1), (project_out, 1, 2), (project_out, 1, 3), (exchange, 1),
        (norm_half, 1, 0), (cube_in, 6), (cube, 8), (norm_half, 1, 1), (project_kv, 2), (halo, 2),
        (cube_more, 8), (cube_in, 7), (project_q, 2), (cube_on, 8), (halo_in, 2), (attention, 2, 0),
        (cube_in, 8), (attention, 2, 1), (attention, 2, 2), (attention, 2, 3), (project_out, 2, 0),
        (project_out, 2, 1), (project_out, 2, 2), (project_out, 2, 3), (exchange, 2),
    )
    for step, *arguments in order:
        step(*arguments)
    for copy in unsent:
        copy.wait_send()


def last_norm(rows, gain, out, done, sems):
    copies = []
    for i in range(4):
        part = pl.ds(i * 32, 32)
        v = rows[part].astype(F32)
        done[part] = v * lax.rsqrt(jnp.mean(v * v, axis=-1, keepdims=True) + EPS) * gain[...]
        copies.append(pltpu.make_async_copy(done.at[part], out.at[part], sems.at[i]))
        copies[-1].start()
    for copy in copies:
        copy.wait()


def shards(inputs, norm_gain, query_weight, key_weight, value_weight, output_weight, sink_logit, final_gain):
    vmem = pl.BlockSpec(memory_space=pltpu.VMEM)
    hbm = pl.BlockSpec(memory_space=pltpu.HBM)
    dma = pltpu.SemaphoreType.DMA
    rows = pl.pallas_call(
        kernel,
        out_shape=jax.ShapeDtypeStruct((BLK, D), BF16),
        in_specs=[hbm] * 7,
        out_specs=vmem,
        scratch_shapes=[
            pltpu.VMEM((LAYERS, D), F32),
            pltpu.VMEM((2, LAYERS), F32),
            pltpu.VMEM((LAYERS, RING, RING, RING, 3 * BLK, BLK), BF16),
            pltpu.VMEM((2 * BLK, D), BF16),
            pltpu.VMEM((LAYERS, 2 * BLK, D), BF16),
            pltpu.VMEM((LAYERS, RING, 4 * BLK, BLK), BF16),
            pltpu.VMEM((RING, 2, 2 * BLK, BLK), BF16),
            pltpu.VMEM((RING, 2 * BLK, BLK), BF16),
            pltpu.VMEM((2 * BLK, D), F32),
            pltpu.VMEM((LAYERS, 2 * BLK, D), BF16),
            pltpu.VMEM((LAYERS, 2 * BLK, D), BF16),
            pltpu.VMEM((2, BLK, 3 * BLK), F32),
            pltpu.VMEM((RING, 8, BLK), F32),
            pltpu.VMEM((8, BLK), F32),
            pltpu.VMEM((4, 2 * BLK, BLK), F32),
            dma((len(SPREADS),)), dma((len(SPREADS),)), dma((2 * len(GROUPS),)), dma((4 * len(GROUPS),)),
            dma((7,)), dma((LAYERS,)), dma((LAYERS,)), dma((LAYERS,)), dma((LAYERS,)), dma((2,)),
        ],
        compiler_params=pltpu.CompilerParams(
            collective_id=0, has_side_effects=True, vmem_limit_bytes=66400000
        ),
    )(
        inputs, query_weight, jnp.swapaxes(key_weight, 1, 2), jnp.swapaxes(value_weight, 1, 2), output_weight,
        norm_gain, jnp.swapaxes(sink_logit, 0, 1),
    )
    return pl.pallas_call(
        last_norm,
        out_shape=jax.ShapeDtypeStruct((BLK, D), F32),
        in_specs=[vmem, vmem],
        out_specs=hbm,
        scratch_shapes=[pltpu.VMEM((BLK, D), F32), dma((4,))],
        compiler_params=pltpu.CompilerParams(vmem_limit_bytes=8 * 1024 * 1024),
    )(rows, final_gain.reshape(1, D))


def solution(mesh):
    in_specs = (
        P("sp", None),
        P(),
        P(None, "sp", "tp"),
        P(None, "sp", "tp"),
        P(None, "sp", "tp"),
        P(None, "sp", "tp"),
        P(None, "tp"),
        P(),
    )
    out_specs = P(("sp", "tp"), None)
    return jax.shard_map(shards, mesh=mesh, in_specs=in_specs, out_specs=out_specs, check_vma=False)
```

```python
import math

import jax
import jax.numpy as jnp
from jax import lax
from jax.experimental import pallas as pl
from jax.experimental.pallas import tpu as pltpu
from jax.sharding import PartitionSpec as P

D = 2048
HEAD_DIM = 64
WINDOW = 128
LAYERS = 3
EPS = 1e-06
BLK = 128
RING = 4
SEQ = 16384
MASKED = -1e30
MESH = pl.DeviceIdType.MESH
F32 = jnp.float32
BF16 = jnp.bfloat16

ROTATIONS = (("x", "y", "z"), ("y", "z", "x"), ("z", "x", "y"))
DIMS = ("x", "z", "y")
KV, Q, O = 0, 1, 2
ROWS = (((0, 48), (48, 96), (96, 128)), ((0, 48), (48, 80), (80, 128)), ((0, 32), (32, 80), (80, 128)))
SPREADS = tuple((kind, lo, hi) for lo, hi in ((0, 1), (1, 3)) for kind in (KV, Q, O))
GROUPS = tuple((kind, layer) for layer in range(LAYERS) for kind in (KV, Q, O))
CHUNKS = 4
LOG2E = 1.4426950408889634


def mod4(v):
    return lax.rem(v + 2 * RING, RING)


def kernel(
    inputs, q_w, k_w, v_w, o_w, norm_gain_in, sink_in,
    out,
    norm_gain, sink_logit, w_all, staged, normed, kv_rows, q_rows, att, part_own, part_send, part_recv, bias, sinks,
    sink_tile, tables,
    spread_send, spread_recv, ring_send, ring_recv, local_sem, halo_send, halo_recv, part_ssem, part_rsem, sink_sem,
):
    sp, tp = lax.axis_index("sp"), lax.axis_index("tp")
    z, y = sp // RING, lax.rem(sp, RING)
    x, c = tp // 2, lax.rem(tp, 2)
    at = {"x": x, "y": y, "z": z}
    chip = sp * RING + x

    def neighbour(dim, step):
        there = dict(at)
        there[dim] = mod4(at[dim] + step)
        return (there["z"] * RING + there["y"], there["x"] * 2 + c)

    def chip_at(step):
        other = lax.rem(chip + step + 64, 64)
        return (other // RING, lax.rem(other, RING) * 2 + c)

    peer = (sp, x * 2 + 1 - c)

    def own_block(first, count):
        return w_all.at[:, x, z, y, pl.ds(first, count)]

    own = [
        pltpu.make_async_copy(k_w, own_block(0, HEAD_DIM), local_sem.at[0]),
        pltpu.make_async_copy(v_w, own_block(HEAD_DIM, HEAD_DIM), local_sem.at[1]),
        pltpu.make_async_copy(q_w, own_block(Q * BLK, BLK), local_sem.at[2]),
        pltpu.make_async_copy(o_w, own_block(O * BLK, BLK), local_sem.at[3]),
    ]
    small = [
        pltpu.make_async_copy(sink_in, sink_logit, local_sem.at[4]),
        pltpu.make_async_copy(norm_gain_in, norm_gain, local_sem.at[5]),
        pltpu.make_async_copy(inputs.at[pl.ds(x * 2 * BLK, 2 * BLK)], staged, local_sem.at[6]),
    ]
    for copy in own + small:
        copy.start()

    barrier = pltpu.get_barrier_semaphore()
    greeted = [neighbour(d, s) for d in DIMS for s in (1, 2, 3)] + [peer]
    for device in greeted:
        pl.semaphore_signal(barrier, inc=1, device_id=device, device_id_type=MESH)
    for copy in own:
        copy.wait()
    pl.semaphore_wait(barrier, len(greeted))

    unsent = []

    def remote(src, dst, ssem, rsem, device):
        return pltpu.make_async_remote_copy(
            src_ref=src, dst_ref=dst, send_sem=ssem, recv_sem=rsem, device_id=device, device_id_type=MESH
        )

    def all_in(ref, sem):
        remote(ref, ref, sem, sem, peer).wait_recv()

    def all_out(ref, sem):
        unsent.append(remote(ref, ref, sem, sem, peer))

    def some_blocks(kind, lo, hi, xs, zs, ys):
        return w_all.at[lo:hi, 0:xs, 0:zs, 0:ys, pl.ds(kind * BLK, BLK)]

    def view(kind, lo, hi, r, phase, pos, half):
        rotation = ROTATIONS[r]
        index = {d: at[d] for d in DIMS}
        index[rotation[phase]] = pos
        for d in rotation[:phase]:
            index[d] = slice(None)
        if half is not None:
            outer = [d for d in DIMS if d in rotation[:phase]][0]
            index[outer] = slice(half * 2, half * 2 + 2)
        first, last = ROWS[kind][r]
        rows = slice(kind * BLK + first, kind * BLK + last)
        return w_all.at[(slice(lo, hi),) + tuple(index[d] for d in DIMS) + (rows,)]

    def spread(i):
        kind, lo, hi = SPREADS[i]
        for r in range(3):
            dim = ROTATIONS[r][0]
            ref = view(kind, lo, hi, r, 0, at[dim], None)
            for step in (1, 3, 2):
                remote(ref, ref, spread_send.at[i], spread_recv.at[i], neighbour(dim, step)).start()
        all_out(some_blocks(kind, lo, hi, 3, 1, 1), spread_send.at[i])

    def spread_in(i):
        kind, lo, hi = SPREADS[i]
        all_in(some_blocks(kind, lo, hi, 3, 1, 1), spread_recv.at[i])

    def hop(group, phase, back, half, slot, step):
        kind, layer = GROUPS[group]
        for r in range(3):
            dim = ROTATIONS[r][phase]
            ref = view(kind, layer, layer + 1, r, phase, mod4(at[dim] + back), half)
            ssem, rsem = ring_send.at[2 * group + phase - 1], ring_recv.at[4 * group + slot]
            remote(ref, ref, ssem, rsem, neighbour(dim, step)).start()

    def landed(group, slot, xs, zs, ys):
        kind, layer = GROUPS[group]
        all_in(some_blocks(kind, layer, layer + 1, xs, zs, ys), ring_recv.at[4 * group + slot])

    def plane(g):
        hop(g, 1, 0, None, 0, 1)
        hop(g, 1, 0, None, 0, -1)

    def plane_on(g):
        landed(g, 0, 2, 1, 4)
        hop(g, 1, -1, 0, 1, 1)
        hop(g, 1, 1, 1, 1, -1)
        kind, layer = GROUPS[g]
        all_out(some_blocks(kind, layer, layer + 1, 3, 1, 4), ring_send.at[2 * g])

    def plane_in(g):
        landed(g, 1, 1, 1, 4)

    def cube(g):
        hop(g, 2, 0, 0, 2, 1)
        hop(g, 2, 0, 1, 2, -1)

    def cube_more(g):
        hop(g, 2, 0, 1, 3, 1)
        hop(g, 2, 0, 0, 3, -1)

    def cube_on(g):
        landed(g, 2, 1, 4, 4)
        hop(g, 2, -1, 0, 3, 1)
        hop(g, 2, 1, 1, 3, -1)
        kind, layer = GROUPS[g]
        all_out(some_blocks(kind, layer, layer + 1, 3, 4, 4), ring_send.at[2 * g + 1])

    def cube_in(g):
        landed(g, 3, 2, 4, 4)

    def norm_rows(src, first, rows, write):
        def body(i, carry):
            at_row = pl.ds(pl.multiple_of(first + i * 16, 16), 16)
            v = src(at_row)
            root = lax.rsqrt(jnp.mean(v * v, axis=-1, keepdims=True) + EPS)
            write(at_row, v * root)
            return carry

        lax.fori_loop(0, rows // 16, body, 0)

    lane = lax.broadcasted_iota(jnp.int32, (2 * BLK, BLK), 1)
    low_half = lax.rem(lane, HEAD_DIM) < HEAD_DIM // 2
    low_head = lane < HEAD_DIM

    def make_tables():
        row = lax.broadcasted_iota(jnp.int32, (2 * BLK, BLK), 0) + chip * 2 * BLK
        place = lax.rem(lane, HEAD_DIM // 2).astype(F32)
        angle = row.astype(F32) * jnp.exp(place * (-math.log(10000.0) * 2 / HEAD_DIM))
        scale = float(D) ** (-0.5)
        cos = jnp.cos(angle) * scale
        sin = jnp.where(low_half, -scale, scale) * jnp.sin(angle)
        tables[0] = cos * (0.125 * LOG2E)
        tables[1] = sin * (0.125 * LOG2E)
        tables[2] = jnp.where(low_head, cos, 1.0)
        tables[3] = jnp.where(low_head, sin, 0.0)

    def make_bias():
        row_i = lax.broadcasted_iota(jnp.int32, (BLK, 3 * BLK), 0)
        col_j = lax.broadcasted_iota(jnp.int32, (BLK, 3 * BLK), 1)
        gap = col_j - row_i
        for b in range(2):
            position = (chip * 2 + b - 1) * BLK + col_j
            allowed = (gap >= 0) & (gap <= 2 * WINDOW) & (position >= 0) & (position < SEQ)
            bias[b] = jnp.where(allowed, 0.0, MASKED)

    def turned(v, which):
        swapped = jnp.where(low_half, pltpu.roll(v, BLK - 32, 1), pltpu.roll(v, 32, 1))
        return v * tables[which] + swapped * tables[which + 1]

    def project_kv(l):
        def body(i, carry):
            w = jnp.concatenate(
                [
                    jnp.concatenate([w_all[l, 2 * i + j, n // RING, n % RING, pl.ds(0, BLK)] for n in range(16)], axis=1)
                    for j in range(2)
                ],
                axis=0,
            )
            raw = lax.dot_general(normed[l], w, (((1,), (1,)), ((), ())), preferred_element_type=F32)
            for j in range(2):
                kv = turned(raw[:, j * BLK : (j + 1) * BLK], 2)
                kv_rows[l, 2 * i + j, pl.ds(BLK, 2 * BLK)] = kv.astype(BF16)
            return carry

        for i in range(2):
            body(i, 0)

    def project_q(l):
        def body(i, carry):
            w = jnp.concatenate(
                [w_all[l, 2 * i + j, :, :, pl.ds(Q * BLK, BLK)].reshape(D, BLK) for j in range(2)], axis=1
            )
            raw = jnp.dot(normed[l], w, preferred_element_type=F32)
            for j in range(2):
                q = turned(raw[:, j * BLK : (j + 1) * BLK], 0)
                head0 = jnp.where(low_head, q, 0.0).astype(BF16)
                head1 = jnp.where(low_head, pltpu.roll(q, HEAD_DIM, 1), 0.0).astype(BF16)
                for b in range(2):
                    q_rows[2 * i + j, b, pl.ds(0, BLK)] = head0[b * BLK : (b + 1) * BLK]
                    q_rows[2 * i + j, b, pl.ds(BLK, BLK)] = head1[b * BLK : (b + 1) * BLK]
            return carry

        for i in range(2):
            body(i, 0)

    def halo(l):
        rows = kv_rows.at[l]
        low, high = pl.ds(BLK, BLK), pl.ds(2 * BLK, BLK)
        sems = halo_send.at[l], halo_recv.at[l]
        remote(rows.at[:, high], rows.at[:, pl.ds(0, BLK)], *sems, chip_at(1)).start()
        remote(rows.at[:, low], rows.at[:, pl.ds(3 * BLK, BLK)], *sems, chip_at(-1)).start()
        all_out(rows.at[:, pl.ds(0, 2 * BLK)], sems[0])

    def halo_in(l):
        all_in(kv_rows.at[l, :, pl.ds(0, 2 * BLK)], halo_recv.at[l])

    low_lane = lax.broadcasted_iota(jnp.int32, (BLK, BLK), 1) < HEAD_DIM
    low_key = lax.broadcasted_iota(jnp.int32, (3 * BLK, BLK), 1) < HEAD_DIM

    def attention(l, h):
        for b in range(2):
            kv = kv_rows[l, h, pl.ds(b * BLK, 3 * BLK)]
            ones_v = jnp.where(low_key, jnp.ones_like(kv), kv)
            s = lax.dot_general(q_rows[h, b], kv, (((1,), (1,)), ((), ())), preferred_element_type=F32)
            sums, extra = [], []
            for g in range(2):
                mine = s[g * BLK : (g + 1) * BLK] + bias[b]
                sink = sinks[h, pl.ds(2 * l + g, 1), pl.ds(0, 1)]
                m = jnp.maximum(jnp.max(mine, axis=1, keepdims=True), sink)
                p = jnp.exp2(mine - m).astype(BF16)
                sums.append(jnp.dot(p, ones_v, preferred_element_type=F32))
                extra.append(jnp.exp2(sink - m))
            top = jnp.where(low_lane, pltpu.roll(sums[0], HEAD_DIM, 1), sums[1])
            below = jnp.where(low_lane, sums[0], pltpu.roll(sums[1], HEAD_DIM, 1))
            below = below + jnp.where(low_lane, extra[0], extra[1])
            att[h, pl.ds(b * BLK, BLK)] = (top / below).astype(BF16)

    def part_rows(l, block):
        return pl.ds(pl.multiple_of(block * BLK, BLK), BLK) if l == LAYERS - 1 else slice(None)

    def send_part(l, j):
        cols = pl.ds(j * (D // CHUNKS), D // CHUNKS)
        rows = part_rows(l, 1 - c)
        remote(
            part_send.at[l, rows, cols], part_recv.at[l, rows, cols], part_ssem.at[l], part_rsem.at[l], peer
        ).start()

    def project_out(l, j):
        lhs = jnp.concatenate([att[h] for h in range(RING)], axis=1)

        def body(i, carry):
            pair = pl.ds(i % 2 * 2, 2)
            w = jnp.concatenate(
                [w_all[l, h, i // 2, pair, pl.ds(O * BLK, BLK)].reshape(2 * BLK, BLK) for h in range(RING)],
                axis=1,
            )
            r = lax.dot_general(lhs, w, (((1,), (1,)), ((), ())), preferred_element_type=F32)
            cols = pl.ds(i * 2 * BLK, 2 * BLK)
            part_own[:, cols] = r
            part_send[l, :, cols] = r.astype(BF16)
            return carry

        for i in (2 * j, 2 * j + 1):
            body(i, 0)
        if j > 0:
            send_part(l, j - 1)

    def parts_in(l):
        all_in(part_recv.at[l, part_rows(l, c)], part_rsem.at[l])

    def exchange(l):
        send_part(l, CHUNKS - 1)
        all_out(part_send.at[l, part_rows(l, 1 - c)], part_ssem.at[l])
        parts_in(l)
        if l == LAYERS - 1:
            mine = part_rows(l, c)
            out[...] = (part_own[mine] + part_recv[l, mine].astype(F32)).astype(BF16)

    def norm_half(l, half):
        gain = norm_gain[pl.ds(l + 1, 1)]

        def state(at_row):
            return (part_own[at_row] + part_recv[l, at_row].astype(F32)).astype(BF16).astype(F32)

        def write_normed(at_row, v):
            normed[l + 1, at_row] = (v * gain).astype(BF16)

        norm_rows(state, half * BLK, BLK, write_normed)

    def first_norm(half):
        gain = norm_gain[pl.ds(0, 1)]

        def write_first(at_row, v):
            normed[0, at_row] = (v * gain).astype(BF16)

        norm_rows(lambda at_row: staged[at_row].astype(F32), half * BLK, BLK, write_first)

    def share_sinks():
        for copy in small:
            copy.wait()
        for l in range(LAYERS):
            for g in range(2):
                sink = jnp.broadcast_to(sink_logit[pl.ds(g, 1), pl.ds(l, 1)], (1, BLK))
                sink_tile[pl.ds(2 * l + g, 1)] = sink * LOG2E
        sinks[x] = sink_tile[...]
        for i in range(1, RING):
            remote(sink_tile, sinks.at[x], sink_sem.at[0], sink_sem.at[1], neighbour("x", i)).start()
        all_out(sinks.at[0:3], sink_sem.at[0])

    def sinks_in():
        all_in(sinks.at[0:3], sink_sem.at[1])

    order = (
        (spread, 1), (spread, 0), (make_bias,), (spread, 2), (spread, 3), (share_sinks,), (first_norm, 0),
        (spread, 5), (spread, 4), (spread_in, 1), (plane, 1), (spread_in, 2), (plane, 2), (spread_in, 0),
        (spread_in, 3), (plane, 0), (spread_in, 5), (plane, 3), (plane, 6), (plane, 5), (plane_on, 0),
        (spread_in, 4), (plane, 4), (make_tables,), (plane_on, 1), (plane, 8), (plane_on, 3), (plane_on, 2),
        (plane_in, 0), (cube, 0), (cube_more, 0), (plane_on, 6), (plane_on, 8), (first_norm, 1), (plane_on, 4),
        (plane_in, 1), (plane_in, 2), (plane_on, 5), (cube_on, 0), (cube, 1), (cube, 2), (cube_more, 1),
        (plane_in, 5), (plane_in, 3), (cube_in, 0), (project_kv, 0), (halo, 0), (cube_on, 1), (cube, 3),
        (cube_more, 2), (cube_on, 2), (plane_in, 4), (cube_in, 1), (cube, 4), (cube_more, 3), (project_q, 0),
        (cube_on, 3), (sinks_in,), (halo_in, 0), (cube_more, 4), (plane, 7), (cube, 5), (attention, 0, 0),
        (attention, 0, 1), (attention, 0, 2), (cube_in, 2), (attention, 0, 3), (project_out, 0, 0),
        (project_out, 0, 1), (project_out, 0, 2), (project_out, 0, 3), (plane_in, 8), (cube_on, 4),
        (exchange, 0), (plane_in, 6), (norm_half, 0, 0), (norm_half, 0, 1), (cube_in, 3), (project_kv, 1),
        (halo, 1), (plane_on, 7), (cube, 6), (cube_more, 5), (cube_on, 5), (plane_in, 7), (cube, 7),
        (cube_in, 4), (project_q, 1), (halo_in, 1), (cube_more, 6), (attention, 1, 0), (cube_on, 6),
        (attention, 1, 1), (attention, 1, 2), (cube_more, 7), (cube_in, 5), (attention, 1, 3), (cube_on, 7),
        (project_out, 1, 0), (project_out, 1, 1), (project_out, 1, 2), (project_out, 1, 3), (exchange, 1),
        (norm_half, 1, 0), (cube_in, 6), (cube, 8), (norm_half, 1, 1), (project_kv, 2), (halo, 2),
        (cube_more, 8), (cube_in, 7), (project_q, 2), (cube_on, 8), (halo_in, 2), (attention, 2, 0),
        (cube_in, 8), (attention, 2, 1), (attention, 2, 2), (attention, 2, 3), (project_out, 2, 0),
        (project_out, 2, 1), (project_out, 2, 2), (project_out, 2, 3), (exchange, 2),
    )
    for step, *arguments in order:
        step(*arguments)
    for copy in unsent:
        copy.wait_send()


def last_norm(rows, gain, out, done, sems):
    copies = []
    for i in range(4):
        part = pl.ds(i * 32, 32)
        v = rows[part].astype(F32)
        done[part] = v * lax.rsqrt(jnp.mean(v * v, axis=-1, keepdims=True) + EPS) * gain[...]
        copies.append(pltpu.make_async_copy(done.at[part], out.at[part], sems.at[i]))
        copies[-1].start()
    for copy in copies:
        copy.wait()


def shards(inputs, norm_gain, query_weight, key_weight, value_weight, output_weight, sink_logit, final_gain):
    vmem = pl.BlockSpec(memory_space=pltpu.VMEM)
    hbm = pl.BlockSpec(memory_space=pltpu.HBM)
    dma = pltpu.SemaphoreType.DMA
    rows = pl.pallas_call(
        kernel,
        out_shape=jax.ShapeDtypeStruct((BLK, D), BF16),
        in_specs=[hbm] * 7,
        out_specs=vmem,
        scratch_shapes=[
            pltpu.VMEM((LAYERS, D), F32),
            pltpu.VMEM((2, LAYERS), F32),
            pltpu.VMEM((LAYERS, RING, RING, RING, 3 * BLK, BLK), BF16),
            pltpu.VMEM((2 * BLK, D), BF16),
            pltpu.VMEM((LAYERS, 2 * BLK, D), BF16),
            pltpu.VMEM((LAYERS, RING, 4 * BLK, BLK), BF16),
            pltpu.VMEM((RING, 2, 2 * BLK, BLK), BF16),
            pltpu.VMEM((RING, 2 * BLK, BLK), BF16),
            pltpu.VMEM((2 * BLK, D), F32),
            pltpu.VMEM((LAYERS, 2 * BLK, D), BF16),
            pltpu.VMEM((LAYERS, 2 * BLK, D), BF16),
            pltpu.VMEM((2, BLK, 3 * BLK), F32),
            pltpu.VMEM((RING, 8, BLK), F32),
            pltpu.VMEM((8, BLK), F32),
            pltpu.VMEM((4, 2 * BLK, BLK), F32),
            dma((len(SPREADS),)), dma((len(SPREADS),)), dma((2 * len(GROUPS),)), dma((4 * len(GROUPS),)),
            dma((7,)), dma((LAYERS,)), dma((LAYERS,)), dma((LAYERS,)), dma((LAYERS,)), dma((2,)),
        ],
        compiler_params=pltpu.CompilerParams(
            collective_id=0, has_side_effects=True, vmem_limit_bytes=66400000
        ),
    )(
        inputs, query_weight, jnp.swapaxes(key_weight, 1, 2), jnp.swapaxes(value_weight, 1, 2), output_weight,
        norm_gain, jnp.swapaxes(sink_logit, 0, 1),
    )
    return pl.pallas_call(
        last_norm,
        out_shape=jax.ShapeDtypeStruct((BLK, D), F32),
        in_specs=[vmem, vmem],
        out_specs=hbm,
        scratch_shapes=[pltpu.VMEM((BLK, D), F32), dma((4,))],
        compiler_params=pltpu.CompilerParams(vmem_limit_bytes=8 * 1024 * 1024),
    )(rows, final_gain.reshape(1, D))


def solution(mesh):
    in_specs = (
        P("sp", None),
        P(),
        P(None, "sp", "tp"),
        P(None, "sp", "tp"),
        P(None, "sp", "tp"),
        P(None, "sp", "tp"),
        P(None, "tp"),
        P(),
    )
    out_specs = P(("sp", "tp"), None)
    return jax.shard_map(shards, mesh=mesh, in_specs=in_specs, out_specs=out_specs, check_vma=False)
```
